512 devices in a mesh: fs: 64 (over z, y), tp: 8 (over x, core).
Axes of the slice: x: 4, y: 4, z: 16, core: 2. Of those that a mesh axis runs over, the one named last changes fastest.
Arguments:
- tokens: bfloat16 [32768, 2048], P('fs', 'tp'), may hold values from -24 to 24
- u_weight: bfloat16 [2048, 1024], P('fs', 'tp'), may hold values from -0.125 to 0.125
- v_weight: bfloat16 [2048, 1024], P('fs', 'tp'), may hold values from -0.125 to 0.125
- sg_gain: float32 [1024], P('tp'), may hold values from 0.1 to 1.9
- spatial_weight: bfloat16 [8, 128, 128], P('tp'), may hold values from -0.5 to 0.5
- spatial_bias: float32 [8, 128], P('tp'), may hold values from 0.1 to 1.9
- out_weight: bfloat16 [1024, 2048], P('tp', 'fs'), may hold values from -0.1875 to 0.1875
- gain_one: float32 [2048], P('tp'), may hold values from 0.1 to 1.9
- gate_weight: bfloat16 [2048, 5632], P('fs', 'tp'), may hold values from -0.125 to 0.125
- up_weight: bfloat16 [2048, 5632], P('fs', 'tp'), may hold values from -0.125 to 0.125
- down_weight: bfloat16 [5632, 2048], P('tp', 'fs'), may hold values from -0.078125 to 0.078125
- gain_two: float32 [2048], P('tp'), may hold values from 0.1 to 1.9
Outputs:
- layer_out: bfloat16 [32768, 2048], P('fs', 'tp')
The draws below stay inside these ranges and needn't reach their ends.
All inputs are finite; a program needn't handle non-finite values.
Results may differ from the reference program's by a relative error of at most 0.014.
Values may be sent and summed in bfloat16 or wider, within the bound.
No kernel may reach another device: no remote copies, remote signals or barrier semaphores. Data moves between devices by JAX's collectives and lax.ppermute only.
A program may use at most 64 MiB of HBM per device.

```python
import math
import jax
import jax.numpy as jnp
from jax import lax

D = 2048
FF = 5632
GROUPS = 8
GROUP_DIM = 128
BLOCK = 128
D_SG = 1024
TOKENS = 32768
N_TP = 8


def draw_tokens(key, part):
    first_key, second_key, third_key = jax.random.split(jax.random.fold_in(key, 11), 3)
    width = D // 16
    scales = jnp.exp(jax.random.uniform(second_key, (16,), jnp.float32, -math.log(4.0), math.log(4.0)))
    base = jax.random.normal(first_key, (TOKENS, D), jnp.float32)
    base = jnp.clip(base, -6.0, 6.0)
    return (base * jnp.repeat(scales, width)[None, :]).astype(jnp.bfloat16)


def steps_of(key, shape, pieces, least, high):
    factor_of, own = 1.0, jax.random.fold_in(key, 6)
    for position, blocks in pieces:
        draws = jnp.exp(jax.random.uniform(jax.random.fold_in(own, position), (blocks,), jnp.float32, least / len(pieces), high / len(pieces)))
        factor_of = factor_of * jnp.repeat(draws, shape[position] // blocks).reshape([-1 if axis == position else 1 for axis in range(len(shape))])
    return factor_of


def bell_draw(rng, extent, deviation, most, shards=(), kind=jnp.bfloat16):
    entries = deviation * jax.random.normal(rng, extent, jnp.float32)
    if shards:
        entries = entries * steps_of(rng, extent, shards, -0.22, 0.18)
    return jnp.clip(entries, -most, most).astype(kind)


def setup_inputs(seed: int = 0) -> dict:
    seeds = jax.random.split(jax.random.key(seed), 13)
    tokens = draw_tokens(jax.random.fold_in(seeds[12], 71), 0)
    u_weight = bell_draw(seeds[1], (D, D_SG), D ** -0.5, 0.125, ((0, 64), (1, 8)))
    v_weight = bell_draw(seeds[2], (D, D_SG), D ** -0.5, 0.125, ((0, 64), (1, 8)))
    sg_gain = jnp.clip(1.0 + 0.18 * jax.random.normal(seeds[3], (D_SG,), jnp.float32), 0.1, 1.9)
    spatial_weight = bell_draw(seeds[4], (GROUPS, BLOCK, BLOCK), BLOCK ** -0.5, 0.5, ((0, 8),))
    spatial_bias = jnp.clip(1.0 + 0.18 * jax.random.normal(seeds[5], (GROUPS, BLOCK), jnp.float32), 0.1, 1.9)
    out_weight = bell_draw(seeds[6], (D_SG, D), D_SG ** -0.5, 0.1875, ((0, 8), (1, 64)))
    gain_one = jnp.clip(1.0 + 0.18 * jax.random.normal(seeds[7], (D,), jnp.float32), 0.1, 1.9)
    gate_weight = bell_draw(seeds[8], (D, FF), D ** -0.5, 0.125, ((0, 64), (1, 8)))
    up_weight = bell_draw(seeds[9], (D, FF), D ** -0.5, 0.125, ((0, 64), (1, 8)))
    down_weight = bell_draw(seeds[10], (FF, D), FF ** -0.5, 0.078125, ((0, 8), (1, 64)))
    gain_two = jnp.clip(1.0 + 0.18 * jax.random.normal(seeds[11], (D,), jnp.float32), 0.1, 1.9)
    return {"tokens": tokens, "u_weight": u_weight, "v_weight": v_weight, "sg_gain": sg_gain, "spatial_weight": spatial_weight, "spatial_bias": spatial_bias, "out_weight": out_weight, "gain_one": gain_one, "gate_weight": gate_weight, "up_weight": up_weight, "down_weight": down_weight, "gain_two": gain_two}


EPS = 1e-05
ALPHA = 2.0 ** 0.25

def norm_rows(vals, gain):
    count = vals.shape[1]
    mean = lax.optimization_barrier(jnp.sum(vals, axis=1, keepdims=True)) / count
    square = lax.optimization_barrier(jnp.sum(vals * vals, axis=1, keepdims=True)) / count
    return (vals - mean) * lax.rsqrt(square - mean * mean + EPS) * gain.astype(jnp.float32)[None, :]

def split_sum(left, weight):
    width = weight.shape[0] // N_TP
    total = jnp.zeros((left.shape[0], weight.shape[1]), jnp.float32)
    for index in range(N_TP):
        part = jnp.dot(left[:, index * width:(index + 1) * width], weight[index * width:(index + 1) * width], preferred_element_type=jnp.float32).astype(jnp.bfloat16)
        part = lax.optimization_barrier(part)
        total = total + part.astype(jnp.float32)
    return total.astype(jnp.bfloat16)

def reference(tokens, u_weight, v_weight, sg_gain, spatial_weight, spatial_bias, out_weight, gain_one, gate_weight, up_weight, down_weight, gain_two):
    gated = jax.nn.gelu(jnp.dot(tokens, u_weight, preferred_element_type=jnp.float32))
    valued = jax.nn.gelu(jnp.dot(tokens, v_weight, preferred_element_type=jnp.float32))
    normed = norm_rows(valued, sg_gain).astype(jnp.bfloat16)
    blocks = TOKENS // BLOCK
    shaped = normed.reshape(blocks, BLOCK, GROUPS, GROUP_DIM).astype(jnp.float32)
    lower = jnp.tril(jnp.ones((BLOCK, BLOCK), jnp.float32))
    masked = spatial_weight.astype(jnp.float32) * lower[None]
    mixed = jnp.einsum('gij,njgd->nigd', masked, shaped)
    mixed = mixed + spatial_bias.astype(jnp.float32).T[None, :, :, None]
    gated_out = (gated * mixed.reshape(TOKENS, D_SG)).astype(jnp.bfloat16)
    mix = split_sum(gated_out, out_weight)
    first = norm_rows(ALPHA * tokens.astype(jnp.float32) + mix.astype(jnp.float32), gain_one).astype(jnp.bfloat16)
    gate = jnp.dot(first, gate_weight, preferred_element_type=jnp.float32)
    upper = jnp.dot(first, up_weight, preferred_element_type=jnp.float32)
    hidden = (jax.nn.silu(gate) * upper).astype(jnp.bfloat16)
    ffn = split_sum(hidden, down_weight)
    layer_out = norm_rows(ALPHA * first.astype(jnp.float32) + ffn.astype(jnp.float32), gain_two)
    return layer_out.astype(jnp.bfloat16)
```

```python
import jax
import jax.numpy as jnp
from jax import lax
from jax.sharding import Mesh
from jax.sharding import PartitionSpec as P

FS = ("z", "y")
TP = ("x", "c")

EPS = 1e-05
ALPHA = 2.0**0.25
BF16 = jnp.bfloat16
F32 = jnp.float32


def sent_to_all(value, axis):
    copies = jnp.broadcast_to(value, (lax.axis_size(axis), *value.shape))
    return lax.all_to_all(copies, axis, split_axis=0, concat_axis=0, tiled=True)


def to_partner(value):
    return lax.ppermute(value, "c", [(0, 1), (1, 0)])


def row_norm(vals, gain):
    count = vals.shape[1]
    mean = jnp.sum(vals, axis=1, keepdims=True) / count
    square = jnp.sum(vals * vals, axis=1, keepdims=True) / count
    return (vals - mean) * lax.rsqrt(square - mean * mean + EPS) * gain[None, :]


def summed_rows(own, other, peers):
    pair = own + to_partner(other.astype(BF16)).astype(F32)
    pieces = pair.astype(BF16).reshape(peers, own.shape[0] // peers, own.shape[1])
    pieces = lax.all_to_all(pieces, "x", 0, 0, tiled=True)
    return jnp.sum(pieces.astype(F32), axis=0)


def on_device(
    tokens,
    u_weight,
    v_weight,
    sg_gain,
    spatial_weight,
    spatial_bias,
    out_weight,
    gain_one,
    gate_weight,
    up_weight,
    down_weight,
    gain_two,
):
    core = lax.axis_index("c")
    chips = lax.axis_size("x")
    cores = lax.axis_size("c")
    parts = chips * cores
    rows, feats = tokens.shape
    width = feats * parts
    sg = u_weight.shape[1]
    ff = gate_weight.shape[1]
    own_rows = rows // parts

    packed = jnp.concatenate([gate_weight, up_weight, down_weight.T], axis=1)
    packed = lax.all_gather(packed, "y", axis=0, tiled=True)
    ffw = lax.all_gather(packed, "z", axis=0, tiled=True)

    small = jnp.concatenate([u_weight, v_weight, out_weight.T], axis=1)
    depth = small.shape[0]
    small = lax.all_gather(small, "z", axis=0, tiled=True)
    small = sent_to_all(small, "y")
    small = small.reshape(small.shape[0], -1, depth, small.shape[2])
    small = jnp.swapaxes(small, 0, 1).reshape(width, small.shape[3])

    gains = sent_to_all(jnp.stack([gain_one, gain_two]), TP)
    gain_1 = gains[:, 0].reshape(width)
    gain_2 = gains[:, 1].reshape(width)

    blocks = sent_to_all(tokens, TP)
    whole = jnp.moveaxis(blocks, 0, 1).reshape(rows, width)
    me = lax.axis_index(TP)
    mine = lax.dynamic_slice_in_dim(blocks, me * own_rows, own_rows, 1)
    mine = jnp.moveaxis(mine, 0, 1).reshape(own_rows, width)

    pre_u = jnp.dot(whole, small[:, :sg], preferred_element_type=F32)
    pre_v = jnp.dot(whole, small[:, sg : 2 * sg], preferred_element_type=F32)
    gated = jax.nn.gelu(pre_u)
    valued = jax.nn.gelu(pre_v)
    sums = jnp.stack([jnp.sum(valued, axis=1), jnp.sum(valued * valued, axis=1)])
    sums = jnp.sum(sent_to_all(sums, TP), axis=0)
    count = sg * parts
    mean = sums[0][:, None] / count
    square = sums[1][:, None] / count
    normed = (valued - mean) * lax.rsqrt(square - mean * mean + EPS) * sg_gain[None, :]
    normed = normed.astype(BF16)

    groups = spatial_weight.shape[0]
    block = spatial_weight.shape[1]
    shaped = normed.reshape(rows // block, block, groups, sg // groups)
    lower = jnp.tril(jnp.ones((block, block), jnp.bool_))
    masked = jnp.where(lower[None], spatial_weight, jnp.zeros_like(spatial_weight))
    mixed = jnp.einsum("gij,njgd->nigd", masked, shaped, preferred_element_type=F32)
    mixed = mixed + spatial_bias.T[None, :, :, None]
    gated_out = (gated * mixed.reshape(rows, sg)).astype(BF16)

    split = gated_out.reshape(chips, cores, own_rows, sg)
    keep = lax.dynamic_index_in_dim(split, core, 1, keepdims=False).reshape(-1, sg)
    give = lax.dynamic_index_in_dim(split, 1 - core, 1, keepdims=False).reshape(-1, sg)
    out_t = small[:, 2 * sg :]
    across = (((1,), (1,)), ((), ()))
    give = lax.dot_general(give, out_t, across, preferred_element_type=F32)
    keep = lax.dot_general(keep, out_t, across, preferred_element_type=F32)
    mix = summed_rows(keep, give, chips).astype(BF16)
    first = row_norm(ALPHA * mine.astype(F32) + mix.astype(F32), gain_1).astype(BF16)

    near = sent_to_all(first, "x").reshape(-1, width)
    far = to_partner(near)
    gate_w, up_w, down_t = ffw[:, :ff], ffw[:, ff : 2 * ff], ffw[:, 2 * ff :]

    def mixer(left):
        gate = jnp.dot(left, gate_w, preferred_element_type=F32)
        upper = jnp.dot(left, up_w, preferred_element_type=F32)
        hidden = (jax.nn.silu(gate) * upper).astype(BF16)
        return lax.dot_general(hidden, down_t, across, preferred_element_type=F32)

    both = mixer(jnp.concatenate([near, far], axis=0))
    half = near.shape[0]
    ffn = summed_rows(both[:half], both[half:], chips).astype(BF16)
    last = row_norm(ALPHA * first.astype(F32) + ffn.astype(F32), gain_2).astype(BF16)
    last = jnp.moveaxis(last.reshape(own_rows, parts, feats), 1, 0)
    return lax.all_to_all(last, TP, 0, 0, tiled=True).reshape(rows, feats)


def solution(mesh):
    tp = mesh.shape["tp"]
    finer = Mesh(mesh.devices.reshape(16, 4, tp // 2, 2), ("z", "y", "x", "c"))
    return jax.shard_map(
        on_device,
        mesh=finer,
        in_specs=(
            P(FS, TP),
            P(FS, TP),
            P(FS, TP),
            P(TP),
            P(TP, None, None),
            P(TP, None),
            P(TP, FS),
            P(TP),
            P(FS, TP),
            P(FS, TP),
            P(TP, FS),
            P(TP),
        ),
        out_specs=P(FS, TP),
        check_vma=False,
    )
```

```python
import jax
import jax.numpy as jnp
from jax import lax
from jax.experimental import pallas as pl
from jax.experimental.pallas import tpu as pltpu
from jax.sharding import Mesh
from jax.sharding import PartitionSpec as P

FS = ("z", "y")
TP = ("x", "c")

EPS = 1e-05
ALPHA = 2.0**0.25
BF16 = jnp.bfloat16
F32 = jnp.float32


def sent_to_all(value, axis):
    copies = jnp.broadcast_to(value, (lax.axis_size(axis), *value.shape))
    return lax.all_to_all(copies, axis, split_axis=0, concat_axis=0, tiled=True)


def to_partner(value):
    return lax.ppermute(value, "c", [(0, 1), (1, 0)])


def summed_rows(own, other, peers):
    pair = own + to_partner(other.astype(BF16)).astype(F32)
    pieces = pair.astype(BF16).reshape(peers, own.shape[0] // peers, own.shape[1])
    return lax.all_to_all(pieces, "x", 0, 0, tiled=True)


def whole_vmem():
    return pl.BlockSpec(memory_space=pltpu.VMEM)


def residual_norm(pieces, base, gain, parts, to_everyone):
    peers, rows, width = pieces.shape

    def body(pieces_ref, base_ref, gain_ref, out_ref):
        added = pieces_ref[0].astype(F32)
        for k in range(1, peers):
            added = added + pieces_ref[k].astype(F32)
        vals = ALPHA * base_ref[...].astype(F32) + added.astype(BF16).astype(F32)
        mean = jnp.sum(vals, axis=1, keepdims=True) / width
        square = jnp.sum(vals * vals, axis=1, keepdims=True) / width
        done = (vals - mean) * lax.rsqrt(square - mean * mean + EPS) * gain_ref[...]
        done = done.astype(BF16)
        for k in range(parts):
            if to_everyone:
                out_ref[k] = done
            else:
                out_ref[k] = done[:, k * (width // parts) : (k + 1) * (width // parts)]

    shape = (parts, rows, width if to_everyone else width // parts)
    return pl.pallas_call(
        body,
        out_shape=jax.ShapeDtypeStruct(shape, BF16),
        in_specs=[whole_vmem()] * 3,
        out_specs=whole_vmem(),
        name="first_norm" if to_everyone else "last_norm",
    )(pieces, base, gain.reshape(1, width))


def packed_ffw(gate, up, down):
    cut = gate.shape[1] // 128 * 128
    return jnp.concatenate([gate[:, :cut], up[:, :cut], gate[:, cut:], up[:, cut:], down.T], axis=1)


def mixer(near, far, ffw, ff):
    half, width = near.shape
    cut = ff // 128 * 128
    tail = ff - cut
    steps = 8
    depth = width // steps
    columns = ffw.shape[1]
    across = (((1,), (1,)), ((), ()))

    def body(near_ref, far_ref, ffw_ref, keep_ref, give_ref, acc, down):
        k = pl.program_id(0)
        at = pl.ds(k * depth, depth)
        weights = ffw_ref[:, : 2 * ff]
        low = jnp.dot(near_ref[:, at], weights, preferred_element_type=F32)
        high = jnp.dot(far_ref[:, at], weights, preferred_element_type=F32)
        down[at, :] = ffw_ref[:, 2 * ff :]

        @pl.when(k == 0)
        def _():
            acc[:half] = low
            acc[half:] = high

        @pl.when(k > 0)
        def _():
            acc[:half] += low
            acc[half:] += high

        @pl.when(k == steps - 1)
        def _():
            def rows(begin, count):
                at = slice(begin, begin + count)
                gate = acc[at, :cut]
                main = (gate * lax.logistic(gate) * acc[at, cut : 2 * cut]).astype(BF16)
                last = acc[at, 2 * cut :]
                ends = (last[:, :tail] * lax.logistic(last[:, :tail]) * last[:, tail:]).astype(BF16)
                out = lax.dot_general(main, down[:, :cut], across, preferred_element_type=F32)
                return out + lax.dot_general(ends, down[:, cut:], across, preferred_element_type=F32)

            give_ref[...] = rows(half, half).astype(BF16)
            keep_ref[...] = rows(0, half)

    return pl.pallas_call(
        body,
        grid=(steps,),
        out_shape=(jax.ShapeDtypeStruct((half, width), F32), jax.ShapeDtypeStruct((half, width), BF16)),
        in_specs=[whole_vmem(), whole_vmem(), pl.BlockSpec((depth, columns), lambda k: (k, 0))],
        out_specs=(whole_vmem(), whole_vmem()),
        scratch_shapes=[pltpu.VMEM((2 * half, 2 * ff), F32), pltpu.VMEM((width, ff), BF16)],
        cost_estimate=pl.CostEstimate(flops=12 * half * width * ff, bytes_accessed=ffw.size * 2, transcendentals=2 * half * ff),
        name="mixer",
    )(near, far, ffw)


def on_device(
    tokens,
    u_weight,
    v_weight,
    sg_gain,
    spatial_weight,
    spatial_bias,
    out_weight,
    gain_one,
    gate_weight,
    up_weight,
    down_weight,
    gain_two,
):
    core = lax.axis_index("c")
    chips = lax.axis_size("x")
    cores = lax.axis_size("c")
    parts = chips * cores
    rows, feats = tokens.shape
    width = feats * parts
    sg = u_weight.shape[1]
    own_rows = rows // parts

    blocks = sent_to_all(tokens, TP)

    packed = lax.all_gather(packed_ffw(gate_weight, up_weight, down_weight), "y", axis=0, tiled=True)
    ffw = lax.all_gather(packed, "z", axis=0, tiled=True)

    small = jnp.concatenate([u_weight, v_weight, out_weight.T], axis=1)
    depth = small.shape[0]
    small = lax.all_gather(small, "z", axis=0, tiled=True)
    small = sent_to_all(small, "y")
    small = small.reshape(small.shape[0], -1, depth, small.shape[2])
    small = jnp.swapaxes(small, 0, 1).reshape(width, small.shape[3])

    whole = jnp.moveaxis(blocks, 0, 1).reshape(rows, width)
    me = lax.axis_index(TP)
    mine = lax.dynamic_slice_in_dim(blocks, me * own_rows, own_rows, 1)
    mine = jnp.moveaxis(mine, 0, 1).reshape(own_rows, width)

    pre_u = jnp.dot(whole, small[:, :sg], preferred_element_type=F32)
    pre_v = jnp.dot(whole, small[:, sg : 2 * sg], preferred_element_type=F32)
    gated = jax.nn.gelu(pre_u)
    valued = jax.nn.gelu(pre_v)
    sums = jnp.stack([jnp.sum(valued, axis=1), jnp.sum(valued * valued, axis=1)])
    gains = jnp.concatenate([gain_one, gain_two]).reshape(-1, rows)
    known = sent_to_all(jnp.concatenate([sums, gains], axis=0), TP)
    gains = known[:, 2:].reshape(parts, 2, feats)
    gain_1 = gains[:, 0].reshape(width)
    gain_2 = gains[:, 1].reshape(width)
    sums = jnp.sum(known[:, :2], axis=0)
    count = sg * parts
    mean = sums[0][:, None] / count
    square = sums[1][:, None] / count
    normed = (valued - mean) * lax.rsqrt(square - mean * mean + EPS) * sg_gain[None, :]
    normed = normed.astype(BF16)

    groups = spatial_weight.shape[0]
    block = spatial_weight.shape[1]
    shaped = normed.reshape(rows // block, block, groups, sg // groups)
    lower = jnp.tril(jnp.ones((block, block), jnp.bool_))
    masked = jnp.where(lower[None], spatial_weight, jnp.zeros_like(spatial_weight))
    mixed = jnp.einsum("gij,njgd->nigd", masked, shaped, preferred_element_type=F32)
    mixed = mixed + spatial_bias.T[None, :, :, None]
    gated_out = (gated * mixed.reshape(rows, sg)).astype(BF16)

    split = gated_out.reshape(chips, cores, own_rows, sg)
    keep = lax.dynamic_index_in_dim(split, core, 1, keepdims=False).reshape(-1, sg)
    give = lax.dynamic_index_in_dim(split, 1 - core, 1, keepdims=False).reshape(-1, sg)
    out_t = small[:, 2 * sg :]
    across = (((1,), (1,)), ((), ()))
    give = lax.dot_general(give, out_t, across, preferred_element_type=F32)
    keep = lax.dot_general(keep, out_t, across, preferred_element_type=F32)
    mix = summed_rows(keep, give, chips)
    first = residual_norm(mix, mine, gain_1, chips, True)

    near = lax.all_to_all(first, "x", 0, 0, tiled=True).reshape(-1, width)
    keep, give = mixer(near, to_partner(near), ffw, gate_weight.shape[1])
    ffn = summed_rows(keep, give, chips)
    last = residual_norm(ffn, first[0], gain_2, parts, False)
    return lax.all_to_all(last, TP, 0, 0, tiled=True).reshape(rows, feats)


def solution(mesh):
    tp = mesh.shape["tp"]
    finer = Mesh(mesh.devices.reshape(16, 4, tp // 2, 2), ("z", "y", "x", "c"))
    return jax.shard_map(
        on_device,
        mesh=finer,
        in_specs=(
            P(FS, TP),
            P(FS, TP),
            P(FS, TP),
            P(TP),
            P(TP, None, None),
            P(TP, None),
            P(TP, FS),
            P(TP),
            P(FS, TP),
            P(FS, TP),
            P(TP, FS),
            P(TP),
        ),
        out_specs=P(FS, TP),
        check_vma=False,
    )
```

```python
import jax
import jax.numpy as jnp
from jax import lax
from jax.experimental import pallas as pl
from jax.experimental.pallas import tpu as pltpu
from jax.sharding import Mesh
from jax.sharding import PartitionSpec as P

FS = ("z", "y")
TP = ("x", "c")

EPS = 1e-05
ALPHA = 2.0**0.25
BF16 = jnp.bfloat16
F32 = jnp.float32
ACROSS = (((1,), (1,)), ((), ()))


def sent_to_all(value, axis):
    copies = jnp.broadcast_to(value, (lax.axis_size(axis), *value.shape))
    return lax.all_to_all(copies, axis, split_axis=0, concat_axis=0, tiled=True)


def to_partner(value):
    return lax.ppermute(value, "c", [(0, 1), (1, 0)])


def row_norm(vals, gain):
    count = vals.shape[1]
    mean = jnp.sum(vals, axis=1, keepdims=True) / count
    square = jnp.sum(vals * vals, axis=1, keepdims=True) / count
    return (vals - mean) * lax.rsqrt(square - mean * mean + EPS) * gain


def summed_rows(own, other, peers):
    pair = own + to_partner(other.astype(BF16)).astype(F32)
    pieces = pair.astype(BF16).reshape(peers, own.shape[0] // peers, own.shape[1])
    return lax.all_to_all(pieces, "x", 0, 0, tiled=True)


def whole_vmem():
    return pl.BlockSpec(memory_space=pltpu.VMEM)


def last_norm(pieces, base, gain, parts):
    peers, rows, width = pieces.shape

    def body(pieces_ref, base_ref, gain_ref, out_ref):
        added = pieces_ref[0].astype(F32)
        for k in range(1, peers):
            added = added + pieces_ref[k].astype(F32)
        vals = ALPHA * base_ref[...].astype(F32) + added.astype(BF16).astype(F32)
        done = row_norm(vals, gain_ref[...]).astype(BF16)
        for k in range(parts):
            out_ref[k] = done[:, k * (width // parts) : (k + 1) * (width // parts)]

    return pl.pallas_call(
        body,
        out_shape=jax.ShapeDtypeStruct((parts, rows, width // parts), BF16),
        in_specs=[whole_vmem()] * 3,
        out_specs=whole_vmem(),
        name="last_norm",
    )(pieces, base, gain.reshape(1, width))


def first_rows(place, gated, blocks, gain, near, far):
    parts, rows, channels = gated.shape
    feats = blocks.shape[2]
    width = parts * feats
    peers = len(near)
    cores = 2
    chips = parts // cores
    depth = 32
    zs = near[0].shape[0] // depth
    wide = near[0].shape[1]
    step = 128

    def body(place_ref, gated_ref, blocks_ref, gain_ref, *rest):
        pieces, out_ref, weights, left, sems = rest[: 2 * peers], rest[-4], rest[-3], rest[-2], rest[-1]
        core = place_ref[0]
        y = place_ref[1]
        copies = []
        for n in range(2 * peers):
            which = core if n < peers else 1 - core
            at = lax.rem(y + 2 * peers - n, peers)
            copies.append(pltpu.make_async_copy(pieces[n], weights.at[which, :, at], sems.at[n]))
        for c in copies:
            c.start()
        for k in range(parts):
            at = (k % cores * chips + k // cores) * channels
            left[:, at : at + channels] = gated_ref[k]
        for c in copies:
            c.wait()
        for r in range(0, rows, step):
            mix = jnp.zeros((step, width), F32)
            for k in range(cores):
                right = weights[k].reshape(width, wide)
                mix += lax.dot_general(left[r : r + step, k * wide : (k + 1) * wide], right, ACROSS, preferred_element_type=F32)
            base = jnp.concatenate([blocks_ref[k, r : r + step] for k in range(parts)], axis=1)
            vals = ALPHA * base.astype(F32) + mix.astype(BF16).astype(F32)
            out_ref[r : r + step] = row_norm(vals, gain_ref[...]).astype(BF16)

    given = [p.reshape(zs, depth, wide) for p in (*near, *far)]
    return pl.pallas_call(
        body,
        out_shape=jax.ShapeDtypeStruct((rows, width), BF16),
        in_specs=[pl.BlockSpec(memory_space=pltpu.SMEM)] + [whole_vmem()] * 3 + [pl.BlockSpec(memory_space=pl.ANY)] * len(given),
        out_specs=whole_vmem(),
        scratch_shapes=[
            pltpu.VMEM((cores, zs, peers, depth, wide), BF16),
            pltpu.VMEM((rows, parts * channels), BF16),
            pltpu.SemaphoreType.DMA((len(given),)),
        ],
        cost_estimate=pl.CostEstimate(flops=2 * rows * width * parts * channels, bytes_accessed=6 << 20, transcendentals=rows),
        name="first_rows",
    )(place, gated, blocks, gain.reshape(1, width), *given)


def packed_weights(gate, up, down):
    cut = gate.shape[1] // 128 * 128
    low = cut - 128
    down = down.T
    big = jnp.concatenate([gate[:, :cut], up[:, :cut], gate[:, cut:], up[:, cut:], down[:, low:]], axis=1)
    return big, down[:, :low]


def mixer(place, first, big, downs, ff):
    rows, width = first.shape
    half = rows // 2
    cut = ff // 128 * 128
    tail = ff - cut
    low = cut - 128
    peers = len(downs)
    depth = 32
    zs = width // peers // depth
    edges = [0, 384, 768, 1152, big.shape[1]]
    chunks = len(edges) - 1

    def body(place_ref, first_ref, big_ref, *rest):
        pieces = rest[:peers]
        keep_ref, give_ref = rest[peers : peers + 2]
        weights = rest[peers + 2 : -3]
        down, acc, sems = rest[-3:]
        core = place_ref[0]
        y = place_ref[1]
        copies = []
        for n in range(chunks):
            at = pl.ds(edges[n], edges[n + 1] - edges[n])
            copies.append(pltpu.make_async_copy(big_ref.at[:, at], weights[n], sems.at[n]))
        for n in range(peers):
            at = lax.rem(y + peers - n, peers)
            copies.append(pltpu.make_async_copy(pieces[n], down.at[:, at], sems.at[chunks + n]))
        for c in copies:
            c.start()
        for n in range(chunks):
            copies[n].wait()
            begin, count = edges[n], min(edges[n + 1], 2 * ff) - edges[n]
            acc[:, begin : begin + count] = jnp.dot(first_ref[...], weights[n][:, :count], preferred_element_type=F32)
        for c in copies[chunks:]:
            c.wait()
        gate = acc[:, :cut]
        main = (gate * lax.logistic(gate) * acc[:, cut : 2 * cut]).astype(BF16)
        last = acc[:, 2 * cut :]
        ends = (last[:, :tail] * lax.logistic(last[:, :tail]) * last[:, tail:]).astype(BF16)
        rest = jnp.concatenate([main[:, low:], ends], axis=1)
        acc_out = lax.dot_general(main[:, :low], down[...].reshape(width, low), ACROSS, preferred_element_type=F32)
        acc_out += lax.dot_general(rest, weights[-1][:, 2 * ff - edges[-2] :], ACROSS, preferred_element_type=F32)

        @pl.when(core == 0)
        def _():
            keep_ref[...] = acc_out[:half]
            give_ref[...] = acc_out[half:].astype(BF16)

        @pl.when(core == 1)
        def _():
            keep_ref[...] = acc_out[half:]
            give_ref[...] = acc_out[:half].astype(BF16)

    given = [p.reshape(zs, depth, p.shape[1]) for p in downs]
    return pl.pallas_call(
        body,
        out_shape=(jax.ShapeDtypeStruct((half, width), F32), jax.ShapeDtypeStruct((half, width), BF16)),
        in_specs=[pl.BlockSpec(memory_space=pltpu.SMEM), whole_vmem()] + [pl.BlockSpec(memory_space=pl.ANY)] * (1 + peers),
        out_specs=(whole_vmem(), whole_vmem()),
        scratch_shapes=[
            *(pltpu.VMEM((width, edges[n + 1] - edges[n]), BF16) for n in range(chunks)),
            pltpu.VMEM((zs, peers, depth, low), BF16),
            pltpu.VMEM((rows, 2 * ff), F32),
            pltpu.SemaphoreType.DMA((chunks + peers,)),
        ],
        cost_estimate=pl.CostEstimate(flops=6 * rows * width * ff, bytes_accessed=12 << 20, transcendentals=rows * ff),
        name="mixer",
    )(place, first, big, *given)


def from_each(value, axis):
    size = lax.axis_size(axis)
    return [value] + [lax.ppermute(value, axis, [(i, (i + k) % size) for i in range(size)]) for k in range(1, size)]


def on_device(
    tokens,
    u_weight,
    v_weight,
    sg_gain,
    spatial_weight,
    spatial_bias,
    out_weight,
    gain_one,
    gate_weight,
    up_weight,
    down_weight,
    gain_two,
):
    core = lax.axis_index("c")
    chips = lax.axis_size("x")
    cores = lax.axis_size("c")
    parts = chips * cores
    rows, feats = tokens.shape
    width = feats * parts
    sg = u_weight.shape[1]
    own_rows = rows // parts

    blocks = sent_to_all(tokens, TP)

    big, rest = packed_weights(gate_weight, up_weight, down_weight)
    big = lax.all_gather(big, "y", axis=0, tiled=True)
    big = lax.all_gather(big, "z", axis=0, tiled=True)

    small = jnp.concatenate([u_weight, v_weight, out_weight.T, rest], axis=1)
    depth = small.shape[0]
    small = lax.all_gather(small, "z", axis=0, tiled=True)
    gates = sent_to_all(small[:, : 2 * sg], "y")
    gates = gates.reshape(gates.shape[0], -1, depth, 2 * sg)
    gates = jnp.swapaxes(gates, 0, 1).reshape(width, 2 * sg)
    out_x = lax.all_gather(small[:, 2 * sg : 3 * sg], "x", axis=1, tiled=True)
    out_near = from_each(out_x, "y")
    out_far = [to_partner(piece) for piece in out_near]
    downs = from_each(small[:, 3 * sg :], "y")

    whole = jnp.moveaxis(blocks, 0, 1).reshape(rows, width)

    pre_u = jnp.dot(whole, gates[:, :sg], preferred_element_type=F32)
    pre_v = jnp.dot(whole, gates[:, sg:], preferred_element_type=F32)
    gated = jax.nn.gelu(pre_u)
    valued = jax.nn.gelu(pre_v)
    sums = jnp.stack([jnp.sum(valued, axis=1), jnp.sum(valued * valued, axis=1)])
    gains = jnp.concatenate([gain_one, gain_two]).reshape(-1, rows)
    known = sent_to_all(jnp.concatenate([sums, gains], axis=0), TP)
    gains = known[:, 2:].reshape(parts, 2, feats)
    gain_1 = gains[:, 0].reshape(width)
    gain_2 = gains[:, 1].reshape(width)
    sums = jnp.sum(known[:, :2], axis=0)
    count = sg * parts
    mean = sums[0][:, None] / count
    square = sums[1][:, None] / count
    normed = (valued - mean) * lax.rsqrt(square - mean * mean + EPS) * sg_gain[None, :]
    normed = normed.astype(BF16)

    groups = spatial_weight.shape[0]
    block = spatial_weight.shape[1]
    shaped = normed.reshape(rows // block, block, groups, sg // groups)
    lower = jnp.tril(jnp.ones((block, block), jnp.bool_))
    masked = jnp.where(lower[None], spatial_weight, jnp.zeros_like(spatial_weight))
    mixed = jnp.einsum("gij,njgd->nigd", masked, shaped, preferred_element_type=F32)
    mixed = mixed + spatial_bias.T[None, :, :, None]
    gated_out = (gated * mixed.reshape(rows, sg)).astype(BF16)

    everyone = sent_to_all(gated_out, TP)
    chip = lax.axis_index("x")
    place = jnp.stack([core, lax.axis_index("y")]).astype(jnp.int32)
    first = first_rows(place, everyone, blocks, gain_1, out_near, out_far)
    keep, give = mixer(place, first, big, downs, gate_weight.shape[1])
    ffn = summed_rows(keep, give, chips)
    mine = lax.dynamic_slice_in_dim(first, (core * chips + chip) * own_rows, own_rows, 0)
    last = last_norm(ffn, mine, gain_2, parts)
    last = lax.all_to_all(last, TP, 0, 0, tiled=True)
    return jnp.swapaxes(last.reshape(chips, cores, own_rows, feats), 0, 1).reshape(rows, feats)


def solution(mesh):
    tp = mesh.shape["tp"]
    finer = Mesh(mesh.devices.reshape(16, 4, tp // 2, 2), ("z", "y", "x", "c"))
    return jax.shard_map(
        on_device,
        mesh=finer,
        in_specs=(
            P(FS, TP),
            P(FS, TP),
            P(FS, TP),
            P(TP),
            P(TP, None, None),
            P(TP, None),
            P(TP, FS),
            P(TP),
            P(FS, TP),
            P(FS, TP),
            P(TP, FS),
            P(TP),
        ),
        out_specs=P(FS, TP),
        check_vma=False,
    )
```

```python
import jax
import jax.numpy as jnp
from jax import lax
from jax.experimental import pallas as pl
from jax.experimental.pallas import tpu as pltpu
from jax.sharding import Mesh
from jax.sharding import PartitionSpec as P

FS = ("z", "y")
TP = ("x", "c")

EPS = 1e-05
ALPHA = 2.0**0.25
BF16 = jnp.bfloat16
F32 = jnp.float32
ACROSS = (((1,), (1,)), ((), ()))


def sent_to_all(value, axis):
    copies = jnp.broadcast_to(value, (lax.axis_size(axis), *value.shape))
    return lax.all_to_all(copies, axis, split_axis=0, concat_axis=0, tiled=True)


def to_partner(value):
    return lax.ppermute(value, "c", [(0, 1), (1, 0)])


def row_norm(vals, gain):
    count = vals.shape[1]
    mean = jnp.sum(vals, axis=1, keepdims=True) / count
    square = jnp.sum(vals * vals, axis=1, keepdims=True) / count
    return (vals - mean) * lax.rsqrt(square - mean * mean + EPS) * gain


def summed_rows(own, other, peers):
    pair = own + to_partner(other.astype(BF16)).astype(F32)
    pieces = pair.astype(BF16).reshape(peers, own.shape[0] // peers, own.shape[1])
    return lax.all_to_all(pieces, "x", 0, 0, tiled=True)


def whole_vmem():
    return pl.BlockSpec(memory_space=pltpu.VMEM)


def last_norm(pieces, base, gain, parts):
    peers, rows, width = pieces.shape

    def body(pieces_ref, base_ref, gain_ref, out_ref):
        added = pieces_ref[0].astype(F32)
        for k in range(1, peers):
            added = added + pieces_ref[k].astype(F32)
        vals = ALPHA * base_ref[...].astype(F32) + added.astype(BF16).astype(F32)
        done = row_norm(vals, gain_ref[...]).astype(BF16)
        for k in range(parts):
            out_ref[k] = done[:, k * (width // parts) : (k + 1) * (width // parts)]

    return pl.pallas_call(
        body,
        out_shape=jax.ShapeDtypeStruct((parts, rows, width // parts), BF16),
        in_specs=[whole_vmem()] * 3,
        out_specs=whole_vmem(),
        name="last_norm",
    )(pieces, base, gain.reshape(1, width))


def first_rows(place, gated, blocks, gain, near, far):
    parts, rows, channels = gated.shape
    feats = blocks.shape[2]
    width = parts * feats
    peers = len(near)
    cores = 2
    chips = parts // cores
    depth = 32
    zs = near[0].shape[0] // depth
    wide = near[0].shape[1]
    deep = zs // parts
    ahead = 3

    def body(place_ref, gated_ref, blocks_ref, gain_ref, *rest):
        pieces = rest[: 2 * peers]
        out_ref, weights, left, base, vals, left_sems, sems = rest[2 * peers :]
        core = place_ref[0]
        y = place_ref[1]
        first = []
        for k in range(parts):
            at = pl.ds((k % cores * chips + k // cores) * channels, channels)
            first.append(pltpu.make_async_copy(gated_ref.at[k], left.at[:, at], left_sems.at[k]))
            first[k].start()
        copies = []
        for j in range(parts):
            at_z = pl.ds(j * deep, deep)
            some = [pltpu.make_async_copy(blocks_ref.at[j], base.at[j], sems.at[j, 2 * peers])]
            for n in range(2 * peers):
                which = core if n < peers else 1 - core
                at_y = lax.rem(y + 2 * peers - n, peers)
                some.append(pltpu.make_async_copy(pieces[n].at[at_z], weights.at[which, at_z, at_y], sems.at[j, n]))
            copies.append(some)
        for some in copies[:ahead]:
            for c in some:
                c.start()
        for c in first:
            c.wait()
        total = jnp.zeros((rows, 1), F32)
        squares = jnp.zeros((rows, 1), F32)
        for j in range(parts):
            for c in copies[j]:
                c.wait()
            if j + ahead < parts:
                for c in copies[j + ahead]:
                    c.start()
            mix = jnp.zeros((rows, feats), F32)
            for k in range(cores):
                right = weights[k, j * deep : (j + 1) * deep].reshape(feats, wide)
                mix += lax.dot_general(left[:, k * wide : (k + 1) * wide], right, ACROSS, preferred_element_type=F32)
            these = ALPHA * base[j].astype(F32) + mix.astype(BF16).astype(F32)
            vals[j] = these
            total += jnp.sum(these, axis=1, keepdims=True)
            squares += jnp.sum(these * these, axis=1, keepdims=True)
        mean = total / width
        scale = lax.rsqrt(squares / width - mean * mean + EPS)
        for j in range(parts):
            at = slice(j * feats, (j + 1) * feats)
            out_ref[:, at] = ((vals[j] - mean) * scale * gain_ref[:, at]).astype(BF16)

    given = [p.reshape(zs, depth, wide) for p in (*near, *far)]
    anywhere = pl.BlockSpec(memory_space=pl.ANY)
    return pl.pallas_call(
        body,
        out_shape=jax.ShapeDtypeStruct((rows, width), BF16),
        in_specs=[pl.BlockSpec(memory_space=pltpu.SMEM), anywhere, anywhere, whole_vmem()] + [anywhere] * len(given),
        out_specs=whole_vmem(),
        scratch_shapes=[
            pltpu.VMEM((cores, zs, peers, depth, wide), BF16),
            pltpu.VMEM((rows, parts * channels), BF16),
            pltpu.VMEM((parts, rows, feats), BF16),
            pltpu.VMEM((parts, rows, feats), F32),
            pltpu.SemaphoreType.DMA((parts,)),
            pltpu.SemaphoreType.DMA((parts, 2 * peers + 1)),
        ],
        cost_estimate=pl.CostEstimate(flops=2 * rows * width * parts * channels, bytes_accessed=9 << 20, transcendentals=rows),
        name="first_rows",
    )(place, gated, blocks, gain.reshape(1, width), *given)


def packed_ffw(gate, up, down):
    cut = gate.shape[1] // 128 * 128
    return jnp.concatenate([gate[:, :cut], up[:, :cut], gate[:, cut:], up[:, cut:], down.T], axis=1)


def mixer(place, first, ffw, ff):
    rows, width = first.shape
    half = rows // 2
    cut = ff // 128 * 128
    tail = ff - cut
    edges = [0, 384, 768, 1152, 2 * ff, 3 * ff]
    spans = [e - b for b, e in zip(edges, edges[1:])]
    chunks = len(spans)
    ahead = 2
    step = 256

    def body(place_ref, first_ref, ffw_ref, keep_ref, give_ref, *rest):
        weights, left, acc, left_sem, sems = rest[:chunks], rest[-4], rest[-3], rest[-2], rest[-1]
        core = place_ref[0]
        copies = []
        for n in range(chunks):
            at = pl.ds(edges[n], spans[n])
            copies.append(pltpu.make_async_copy(ffw_ref.at[:, at], weights[n], sems.at[n]))
        lead = pltpu.make_async_copy(first_ref, left, left_sem.at[0])
        lead.start()
        for c in copies[:ahead]:
            c.start()
        lead.wait()
        for n in range(chunks - 1):
            copies[n].wait()
            if n + ahead < chunks:
                copies[n + ahead].start()
            acc[:, edges[n] : edges[n + 1]] = jnp.dot(left[...], weights[n][...], preferred_element_type=F32)
        gate = acc[:, :cut]
        main = (gate * lax.logistic(gate) * acc[:, cut : 2 * cut]).astype(BF16)
        last = acc[:, 2 * cut :]
        ends = (last[:, :tail] * lax.logistic(last[:, :tail]) * last[:, tail:]).astype(BF16)
        hidden = jnp.concatenate([main, ends], axis=1)
        copies[-1].wait()

        def out(keep_at, give_at):
            for b in range(0, width, step):
                done = lax.dot_general(hidden, weights[-1][b : b + step], ACROSS, preferred_element_type=F32)
                keep_ref[:, b : b + step] = done[keep_at : keep_at + half]
                give_ref[:, b : b + step] = done[give_at : give_at + half].astype(BF16)

        @pl.when(core == 0)
        def _():
            out(0, half)

        @pl.when(core == 1)
        def _():
            out(half, 0)

    anywhere = pl.BlockSpec(memory_space=pl.ANY)
    return pl.pallas_call(
        body,
        out_shape=(jax.ShapeDtypeStruct((half, width), F32), jax.ShapeDtypeStruct((half, width), BF16)),
        in_specs=[pl.BlockSpec(memory_space=pltpu.SMEM), anywhere, anywhere],
        out_specs=(whole_vmem(), whole_vmem()),
        scratch_shapes=[
            *(pltpu.VMEM((width, n), BF16) for n in spans),
            pltpu.VMEM((rows, width), BF16),
            pltpu.VMEM((rows, 2 * ff), F32),
            pltpu.SemaphoreType.DMA((1,)),
            pltpu.SemaphoreType.DMA((chunks,)),
        ],
        cost_estimate=pl.CostEstimate(flops=6 * rows * width * ff, bytes_accessed=14 << 20, transcendentals=rows * ff),
        name="mixer",
    )(place, first, ffw)


def from_each(value, axis):
    size = lax.axis_size(axis)
    return [value] + [lax.ppermute(value, axis, [(i, (i + k) % size) for i in range(size)]) for k in range(1, size)]


def on_device(
    tokens,
    u_weight,
    v_weight,
    sg_gain,
    spatial_weight,
    spatial_bias,
    out_weight,
    gain_one,
    gate_weight,
    up_weight,
    down_weight,
    gain_two,
):
    core = lax.axis_index("c")
    chips = lax.axis_size("x")
    cores = lax.axis_size("c")
    parts = chips * cores
    rows, feats = tokens.shape
    width = feats * parts
    sg = u_weight.shape[1]
    own_rows = rows // parts

    blocks = sent_to_all(tokens, TP)

    ffw = lax.all_gather(packed_ffw(gate_weight, up_weight, down_weight), "y", axis=0, tiled=True)
    ffw = lax.all_gather(ffw, "z", axis=0, tiled=True)

    small = jnp.concatenate([u_weight, v_weight, out_weight.T], axis=1)
    depth = small.shape[0]
    small = lax.all_gather(small, "z", axis=0, tiled=True)
    gates = sent_to_all(small[:, : 2 * sg], "y")
    gates = gates.reshape(gates.shape[0], -1, depth, 2 * sg)
    gates = jnp.swapaxes(gates, 0, 1).reshape(width, 2 * sg)
    out_x = lax.all_gather(small[:, 2 * sg :], "x", axis=1, tiled=True)
    out_near = from_each(out_x, "y")
    out_far = [to_partner(piece) for piece in out_near]

    whole = jnp.moveaxis(blocks, 0, 1).reshape(rows, width)

    pre_u = jnp.dot(whole, gates[:, :sg], preferred_element_type=F32)
    pre_v = jnp.dot(whole, gates[:, sg:], preferred_element_type=F32)
    gated = jax.nn.gelu(pre_u)
    valued = jax.nn.gelu(pre_v)
    sums = jnp.stack([jnp.sum(valued, axis=1), jnp.sum(valued * valued, axis=1)])
    gains = jnp.concatenate([gain_one, gain_two]).reshape(-1, rows)
    known = sent_to_all(jnp.concatenate([sums, gains], axis=0), TP)
    gains = known[:, 2:].reshape(parts, 2, feats)
    gain_1 = gains[:, 0].reshape(width)
    gain_2 = gains[:, 1].reshape(width)
    sums = jnp.sum(known[:, :2], axis=0)
    count = sg * parts
    mean = sums[0][:, None] / count
    square = sums[1][:, None] / count
    normed = (valued - mean) * lax.rsqrt(square - mean * mean + EPS) * sg_gain[None, :]
    normed = normed.astype(BF16)

    groups = spatial_weight.shape[0]
    block = spatial_weight.shape[1]
    shaped = normed.reshape(rows // block, block, groups, sg // groups)
    lower = jnp.tril(jnp.ones((block, block), jnp.bool_))
    masked = jnp.where(lower[None], spatial_weight, jnp.zeros_like(spatial_weight))
    mixed = jnp.einsum("gij,njgd->nigd", masked, shaped, preferred_element_type=F32)
    mixed = mixed + spatial_bias.T[None, :, :, None]
    gated_out = (gated * mixed.reshape(rows, sg)).astype(BF16)

    everyone = sent_to_all(gated_out, TP)
    chip = lax.axis_index("x")
    place = jnp.stack([core, lax.axis_index("y")]).astype(jnp.int32)
    first = first_rows(place, everyone, blocks, gain_1, out_near, out_far)
    keep, give = mixer(place, first, ffw, gate_weight.shape[1])
    ffn = summed_rows(keep, give, chips)
    mine = lax.dynamic_slice_in_dim(first, (core * chips + chip) * own_rows, own_rows, 0)
    last = last_norm(ffn, mine, gain_2, parts)
    last = lax.all_to_all(last, TP, 0, 0, tiled=True)
    return jnp.swapaxes(last.reshape(chips, cores, own_rows, feats), 0, 1).reshape(rows, feats)


def solution(mesh):
    tp = mesh.shape["tp"]
    finer = Mesh(mesh.devices.reshape(16, 4, tp // 2, 2), ("z", "y", "x", "c"))
    return jax.shard_map(
        on_device,
        mesh=finer,
        in_specs=(
            P(FS, TP),
            P(FS, TP),
            P(FS, TP),
            P(TP),
            P(TP, None, None),
            P(TP, None),
            P(TP, FS),
            P(TP),
            P(FS, TP),
            P(FS, TP),
            P(TP, FS),
            P(TP),
        ),
        out_specs=P(FS, TP),
        check_vma=False,
    )
```

```python
import jax
import jax.numpy as jnp
from jax import lax
from jax.experimental import pallas as pl
from jax.experimental.pallas import tpu as pltpu
from jax.sharding import Mesh
from jax.sharding import PartitionSpec as P

FS = ("z", "y")
TP = ("x", "c")

EPS = 1e-05
ALPHA = 2.0**0.25
BF16 = jnp.bfloat16
F32 = jnp.float32
ACROSS = (((1,), (1,)), ((), ()))


def sent_to_all(value, axis):
    copies = jnp.broadcast_to(value, (lax.axis_size(axis), *value.shape))
    return lax.all_to_all(copies, axis, split_axis=0, concat_axis=0, tiled=True)


def to_partner(value):
    return lax.ppermute(value, "c", [(0, 1), (1, 0)])


def row_norm(vals, gain):
    count = vals.shape[1]
    mean = jnp.sum(vals, axis=1, keepdims=True) / count
    square = jnp.sum(vals * vals, axis=1, keepdims=True) / count
    return (vals - mean) * lax.rsqrt(square - mean * mean + EPS) * gain


def whole_vmem():
    return pl.BlockSpec(memory_space=pltpu.VMEM)


def last_norm(pieces, base, gain, parts):
    peers, rows, width = pieces.shape

    def body(pieces_ref, base_ref, gain_ref, out_ref):
        added = pieces_ref[0].astype(F32)
        for k in range(1, peers):
            added = added + pieces_ref[k].astype(F32)
        vals = ALPHA * base_ref[...].astype(F32) + added.astype(BF16).astype(F32)
        done = row_norm(vals, gain_ref[...]).astype(BF16)
        for k in range(parts):
            out_ref[k] = done[:, k * (width // parts) : (k + 1) * (width // parts)]

    return pl.pallas_call(
        body,
        out_shape=jax.ShapeDtypeStruct((parts, rows, width // parts), BF16),
        in_specs=[whole_vmem()] * 3,
        out_specs=whole_vmem(),
        name="last_norm",
    )(pieces, base, gain.reshape(1, width))


def projected(place, gated, pieces):
    chips, rows, channels = gated.shape
    peers = len(pieces)
    depth = 32
    zs = pieces[0].shape[0] // depth
    wide = pieces[0].shape[1]
    width = zs * peers * depth
    steps = 8
    deep = zs // steps
    span = width // steps
    ahead = 3

    def body(place_ref, gated_ref, *rest):
        pieces = rest[:peers]
        out_ref, weights, left, left_sems, sems = rest[peers:]
        y = place_ref[2]
        first = []
        for k in range(chips):
            first.append(pltpu.make_async_copy(gated_ref.at[k], left.at[:, pl.ds(k * channels, channels)], left_sems.at[k]))
            first[k].start()
        copies = []
        for j in range(steps):
            at_z = pl.ds(j * deep, deep)
            some = []
            for n in range(peers):
                at_y = lax.rem(y + peers - n, peers)
                some.append(pltpu.make_async_copy(pieces[n].at[at_z], weights.at[at_z, at_y], sems.at[j, n]))
            copies.append(some)
        for some in copies[:ahead]:
            for c in some:
                c.start()
        for c in first:
            c.wait()
        for j in range(steps):
            for c in copies[j]:
                c.wait()
            if j + ahead < steps:
                for c in copies[j + ahead]:
                    c.start()
            right = weights[j * deep : (j + 1) * deep].reshape(span, wide)
            part = lax.dot_general(left[...], right, ACROSS, preferred_element_type=F32)
            out_ref[:, j * span : (j + 1) * span] = part.astype(BF16)

    given = [p.reshape(zs, depth, wide) for p in pieces]
    anywhere = pl.BlockSpec(memory_space=pl.ANY)
    return pl.pallas_call(
        body,
        out_shape=jax.ShapeDtypeStruct((rows, width), BF16),
        in_specs=[pl.BlockSpec(memory_space=pltpu.SMEM)] + [anywhere] * (1 + peers),
        out_specs=whole_vmem(),
        scratch_shapes=[
            pltpu.VMEM((zs, peers, depth, wide), BF16),
            pltpu.VMEM((rows, chips * channels), BF16),
            pltpu.SemaphoreType.DMA((chips,)),
            pltpu.SemaphoreType.DMA((steps, peers)),
        ],
        cost_estimate=pl.CostEstimate(flops=2 * rows * width * wide, bytes_accessed=6 << 20, transcendentals=0),
        name="projected",
    )(place, gated, *given)


def mixer(place, own, other, blocks, gain, ffw, ff):
    rows, width = own.shape
    parts, _, feats = blocks.shape
    chips = parts // 2
    half = rows // 2
    few = rows // parts
    edges = [0, 384, 768, 1152, 2 * ff, 3 * ff]
    spans = [e - b for b, e in zip(edges, edges[1:])]
    chunks = len(spans)
    ahead = 2
    step = 256

    def body(place_ref, own_ref, other_ref, blocks_ref, gain_ref, ffw_ref, mine_ref, keep_ref, give_ref, *rest):
        weights = rest[:chunks]
        base, low, high, vals, left, acc, in_sems, sems = rest[chunks:]
        core = place_ref[0]
        me = place_ref[1]
        inputs = []
        for j in range(parts):
            at = pl.ds(j * feats, feats)
            inputs.append(
                [
                    pltpu.make_async_copy(own_ref.at[:, at], low.at[j], in_sems.at[j, 0]),
                    pltpu.make_async_copy(other_ref.at[:, at], high.at[j], in_sems.at[j, 1]),
                    pltpu.make_async_copy(blocks_ref.at[j], base.at[j], in_sems.at[j, 2]),
                ]
            )
            for c in inputs[j]:
                c.start()
        copies = []
        for n in range(chunks):
            at = pl.ds(edges[n], spans[n])
            copies.append(pltpu.make_async_copy(ffw_ref.at[:, at], weights[n], sems.at[n]))
        for c in copies[:ahead]:
            c.start()
        total = jnp.zeros((rows, 1), F32)
        squares = jnp.zeros((rows, 1), F32)
        for j in range(parts):
            for c in inputs[j]:
                c.wait()
            mix = (low[j].astype(F32) + high[j].astype(F32)).astype(BF16)
            these = ALPHA * base[j].astype(F32) + mix.astype(F32)
            vals[j] = these
            total += jnp.sum(these, axis=1, keepdims=True)
            squares += jnp.sum(these * these, axis=1, keepdims=True)
        mean = total / width
        scale = lax.rsqrt(squares / width - mean * mean + EPS)
        for j in range(parts):
            at = slice(j * feats, (j + 1) * feats)
            left[:, at] = ((vals[j] - mean) * scale * gain_ref[:, at]).astype(BF16)
        mine_ref[...] = left[pl.ds(pl.multiple_of(me * few, few), few), :]
        for n in range(chunks - 1):
            copies[n].wait()
            if n + ahead < chunks:
                copies[n + ahead].start()
            acc[:, edges[n] : edges[n + 1]] = jnp.dot(left[...], weights[n][...], preferred_element_type=F32)
        gate = acc[:, :ff]
        hidden = (gate * lax.logistic(gate) * acc[:, ff:]).astype(BF16)
        copies[-1].wait()

        def out(keep_core):
            for b in range(0, width, step):
                done = lax.dot_general(hidden, weights[-1][b : b + step], ACROSS, preferred_element_type=F32).astype(BF16)
                for x in range(chips):
                    here = slice(x * few, (x + 1) * few)
                    keep = (2 * x + keep_core) * few
                    give = (2 * x + 1 - keep_core) * few
                    keep_ref[here, b : b + step] = done[keep : keep + few]
                    give_ref[here, b : b + step] = done[give : give + few]

        @pl.when(core == 0)
        def _():
            out(0)

        @pl.when(core == 1)
        def _():
            out(1)

    anywhere = pl.BlockSpec(memory_space=pl.ANY)
    return pl.pallas_call(
        body,
        out_shape=(
            jax.ShapeDtypeStruct((few, width), BF16),
            jax.ShapeDtypeStruct((half, width), BF16),
            jax.ShapeDtypeStruct((half, width), BF16),
        ),
        in_specs=[pl.BlockSpec(memory_space=pltpu.SMEM), anywhere, anywhere, anywhere, whole_vmem(), anywhere],
        out_specs=(whole_vmem(),) * 3,
        scratch_shapes=[
            *(pltpu.VMEM((width, n), BF16) for n in spans),
            pltpu.VMEM((parts, rows, feats), BF16),
            pltpu.VMEM((parts, rows, feats), BF16),
            pltpu.VMEM((parts, rows, feats), BF16),
            pltpu.VMEM((parts, rows, feats), F32),
            pltpu.VMEM((rows, width), BF16),
            pltpu.VMEM((rows, 2 * ff), F32),
            pltpu.SemaphoreType.DMA((parts, 3)),
            pltpu.SemaphoreType.DMA((chunks,)),
        ],
        cost_estimate=pl.CostEstimate(flops=6 * rows * width * ff, bytes_accessed=18 << 20, transcendentals=rows * ff),
        name="mixer",
    )(place, own, other, blocks, gain.reshape(1, width), ffw)


def from_each(value, axis):
    size = lax.axis_size(axis)
    return [value] + [lax.ppermute(value, axis, [(i, (i + k) % size) for i in range(size)]) for k in range(1, size)]


def on_device(
    tokens,
    u_weight,
    v_weight,
    sg_gain,
    spatial_weight,
    spatial_bias,
    out_weight,
    gain_one,
    gate_weight,
    up_weight,
    down_weight,
    gain_two,
):
    core = lax.axis_index("c")
    chips = lax.axis_size("x")
    parts = chips * lax.axis_size("c")
    rows, feats = tokens.shape
    width = feats * parts
    sg = u_weight.shape[1]
    own_rows = rows // parts

    blocks = sent_to_all(tokens, TP)

    ffw = lax.all_gather(jnp.concatenate([gate_weight, up_weight, down_weight.T], axis=1), "y", axis=0, tiled=True)
    ffw = lax.all_gather(ffw, "z", axis=0, tiled=True)

    small = jnp.concatenate([u_weight, v_weight, out_weight.T], axis=1)
    depth = small.shape[0]
    small = lax.all_gather(small, "z", axis=0, tiled=True)
    gates = sent_to_all(small[:, : 2 * sg], "y")
    gates = gates.reshape(gates.shape[0], -1, depth, 2 * sg)
    gates = jnp.swapaxes(gates, 0, 1).reshape(width, 2 * sg)
    out_x = lax.all_gather(small[:, 2 * sg :], "x", axis=1, tiled=True)
    out_rows = from_each(out_x, "y")

    whole = jnp.moveaxis(blocks, 0, 1).reshape(rows, width)

    pre_u = jnp.dot(whole, gates[:, :sg], preferred_element_type=F32)
    pre_v = jnp.dot(whole, gates[:, sg:], preferred_element_type=F32)
    gated = jax.nn.gelu(pre_u)
    valued = jax.nn.gelu(pre_v)
    sums = jnp.stack([jnp.sum(valued, axis=1), jnp.sum(valued * valued, axis=1)])
    gains = jnp.concatenate([gain_one, gain_two]).reshape(-1, rows)
    known = sent_to_all(jnp.concatenate([sums, gains], axis=0), TP)
    gains = known[:, 2:].reshape(parts, 2, feats)
    gain_1 = gains[:, 0].reshape(width)
    gain_2 = gains[:, 1].reshape(width)
    sums = jnp.sum(known[:, :2], axis=0)
    count = sg * parts
    mean = sums[0][:, None] / count
    square = sums[1][:, None] / count
    normed = (valued - mean) * lax.rsqrt(square - mean * mean + EPS) * sg_gain[None, :]
    normed = normed.astype(BF16)

    groups = spatial_weight.shape[0]
    block = spatial_weight.shape[1]
    shaped = normed.reshape(rows // block, block, groups, sg // groups)
    lower = jnp.tril(jnp.ones((block, block), jnp.bool_))
    masked = jnp.where(lower[None], spatial_weight, jnp.zeros_like(spatial_weight))
    mixed = jnp.einsum("gij,njgd->nigd", masked, shaped, preferred_element_type=F32)
    mixed = mixed + spatial_bias.T[None, :, :, None]
    gated_out = (gated * mixed.reshape(rows, sg)).astype(BF16)

    together = sent_to_all(gated_out, "x")
    place = jnp.stack([core, lax.axis_index(TP), lax.axis_index("y")]).astype(jnp.int32)
    own = projected(place, together, out_rows)
    mine, keep, give = mixer(place, own, to_partner(own), blocks, gain_1, ffw, gate_weight.shape[1])
    pair = (keep.astype(F32) + to_partner(give).astype(F32)).astype(BF16)
    pieces = lax.all_to_all(pair.reshape(chips, own_rows, width), "x", 0, 0, tiled=True)
    last = last_norm(pieces, mine, gain_2, parts)
    return lax.all_to_all(last, TP, 0, 0, tiled=True).reshape(rows, feats)


def solution(mesh):
    tp = mesh.shape["tp"]
    finer = Mesh(mesh.devices.reshape(16, 4, tp // 2, 2), ("z", "y", "x", "c"))
    return jax.shard_map(
        on_device,
        mesh=finer,
        in_specs=(
            P(FS, TP),
            P(FS, TP),
            P(FS, TP),
            P(TP),
            P(TP, None, None),
            P(TP, None),
            P(TP, FS),
            P(TP),
            P(FS, TP),
            P(FS, TP),
            P(TP, FS),
            P(TP),
        ),
        out_specs=P(FS, TP),
        check_vma=False,
    )
```

```python
import jax
import jax.numpy as jnp
from jax import lax
from jax.experimental import pallas as pl
from jax.experimental.pallas import tpu as pltpu
from jax.sharding import Mesh
from jax.sharding import PartitionSpec as P

FS = ("z", "y")
TP = ("x", "c")

EPS = 1e-05
ALPHA = 2.0**0.25
BF16 = jnp.bfloat16
F32 = jnp.float32
ACROSS = (((1,), (1,)), ((), ()))


def sent_to_all(value, axis):
    copies = jnp.broadcast_to(value, (lax.axis_size(axis), *value.shape))
    return lax.all_to_all(copies, axis, split_axis=0, concat_axis=0, tiled=True)


def to_partner(value):
    return lax.ppermute(value, "c", [(0, 1), (1, 0)])


def row_norm(vals, gain):
    count = vals.shape[1]
    mean = jnp.sum(vals, axis=1, keepdims=True) / count
    square = jnp.sum(vals * vals, axis=1, keepdims=True) / count
    return (vals - mean) * lax.rsqrt(square - mean * mean + EPS) * gain


def in_vmem(value):
    return pltpu.with_memory_space_constraint(value, pltpu.VMEM)


def in_hbm(value):
    return pltpu.with_memory_space_constraint(value, pltpu.HBM)


def whole_vmem():
    return pl.BlockSpec(memory_space=pltpu.VMEM)


def last_norm(pieces, base, gain, parts):
    peers, rows, width = pieces.shape

    def body(pieces_ref, base_ref, gain_ref, out_ref):
        added = pieces_ref[0].astype(F32)
        for k in range(1, peers):
            added = added + pieces_ref[k].astype(F32)
        vals = ALPHA * base_ref[...].astype(F32) + added.astype(BF16).astype(F32)
        done = row_norm(vals, gain_ref[...]).astype(BF16)
        for k in range(parts):
            out_ref[k] = done[:, k * (width // parts) : (k + 1) * (width // parts)]

    return pl.pallas_call(
        body,
        out_shape=pltpu.VMEM((parts, rows, width // parts), BF16),
        in_specs=[whole_vmem()] * 3,
        out_specs=whole_vmem(),
        name="last_norm",
    )(in_vmem(pieces), in_vmem(base), gain.reshape(1, width))


def projected(place, gated, pieces):
    chips, rows, channels = gated.shape
    peers = len(pieces)
    depth = 32
    zs = pieces[0].shape[0] // depth
    wide = pieces[0].shape[1]
    width = zs * peers * depth
    steps = 8
    deep = zs // steps
    span = width // steps
    ahead = 3

    def body(place_ref, gated_ref, *rest):
        pieces = rest[:peers]
        out_ref, weights, left, sems = rest[peers:]
        y = place_ref[2]
        copies = []
        for j in range(steps):
            at_z = pl.ds(j * deep, deep)
            some = []
            for n in range(peers):
                at_y = lax.rem(y + peers - n, peers)
                some.append(pltpu.make_async_copy(pieces[n].at[at_z], weights.at[at_z, at_y], sems.at[j, n]))
            copies.append(some)
        for some in copies[:ahead]:
            for c in some:
                c.start()
        for k in range(chips):
            left[:, k * channels : (k + 1) * channels] = gated_ref[k]
        for j in range(steps):
            for c in copies[j]:
                c.wait()
            if j + ahead < steps:
                for c in copies[j + ahead]:
                    c.start()
            right = weights[j * deep : (j + 1) * deep].reshape(span, wide)
            part = lax.dot_general(left[...], right, ACROSS, preferred_element_type=F32)
            out_ref[:, j * span : (j + 1) * span] = part.astype(BF16)

    given = [p.reshape(zs, depth, wide) for p in pieces]
    anywhere = pl.BlockSpec(memory_space=pl.ANY)
    return pl.pallas_call(
        body,
        out_shape=jax.ShapeDtypeStruct((rows, width), BF16),
        in_specs=[pl.BlockSpec(memory_space=pltpu.SMEM), whole_vmem()] + [anywhere] * peers,
        out_specs=whole_vmem(),
        scratch_shapes=[
            pltpu.VMEM((zs, peers, depth, wide), BF16),
            pltpu.VMEM((rows, chips * channels), BF16),
            pltpu.SemaphoreType.DMA((steps, peers)),
        ],
        cost_estimate=pl.CostEstimate(flops=2 * rows * width * wide, bytes_accessed=6 << 20, transcendentals=0),
        name="projected",
    )(in_hbm(place), in_vmem(gated), *given)


def mixer(place, own, other, blocks, gain, ffw, ff):
    rows, width = own.shape
    parts, _, feats = blocks.shape
    chips = parts // 2
    half = rows // 2
    few = rows // parts
    edges = [0, 384, 768, 1152, 2 * ff, 3 * ff]
    spans = [e - b for b, e in zip(edges, edges[1:])]
    chunks = len(spans)
    ahead = 2
    step = 256

    def body(place_ref, own_ref, other_ref, blocks_ref, gain_ref, ffw_ref, mine_ref, keep_ref, give_ref, *rest):
        weights = rest[:chunks]
        base, low, vals, left, acc, in_sems, sems = rest[chunks:]
        core = place_ref[0]
        me = place_ref[1]
        inputs = []
        for j in range(parts):
            at = pl.ds(j * feats, feats)
            inputs.append(
                [
                    pltpu.make_async_copy(own_ref.at[:, at], low.at[j], in_sems.at[j, 0]),
                    pltpu.make_async_copy(blocks_ref.at[j], base.at[j], in_sems.at[j, 1]),
                ]
            )
            for c in inputs[j]:
                c.start()
        copies = []
        for n in range(chunks):
            at = pl.ds(edges[n], spans[n])
            copies.append(pltpu.make_async_copy(ffw_ref.at[:, at], weights[n], sems.at[n]))
        for c in copies[:ahead]:
            c.start()
        total = jnp.zeros((rows, 1), F32)
        squares = jnp.zeros((rows, 1), F32)
        for j in range(parts):
            for c in inputs[j]:
                c.wait()
            high = other_ref[:, j * feats : (j + 1) * feats]
            mix = (low[j].astype(F32) + high.astype(F32)).astype(BF16)
            these = ALPHA * base[j].astype(F32) + mix.astype(F32)
            vals[j] = these
            total += jnp.sum(these, axis=1, keepdims=True)
            squares += jnp.sum(these * these, axis=1, keepdims=True)
        mean = total / width
        scale = lax.rsqrt(squares / width - mean * mean + EPS)
        for j in range(parts):
            at = slice(j * feats, (j + 1) * feats)
            left[:, at] = ((vals[j] - mean) * scale * gain_ref[:, at]).astype(BF16)
        mine_ref[...] = left[pl.ds(pl.multiple_of(me * few, few), few), :]
        for n in range(chunks - 1):
            copies[n].wait()
            if n + ahead < chunks:
                copies[n + ahead].start()
            acc[:, edges[n] : edges[n + 1]] = jnp.dot(left[...], weights[n][...], preferred_element_type=F32)
        gate = acc[:, :ff]
        hidden = (gate * lax.logistic(gate) * acc[:, ff:]).astype(BF16)
        copies[-1].wait()

        def out(keep_core):
            for b in range(0, width, step):
                done = lax.dot_general(hidden, weights[-1][b : b + step], ACROSS, preferred_element_type=F32).astype(BF16)
                for x in range(chips):
                    here = slice(x * few, (x + 1) * few)
                    keep = (2 * x + keep_core) * few
                    give = (2 * x + 1 - keep_core) * few
                    keep_ref[here, b : b + step] = done[keep : keep + few]
                    give_ref[here, b : b + step] = done[give : give + few]

        @pl.when(core == 0)
        def _():
            out(0)

        @pl.when(core == 1)
        def _():
            out(1)

    anywhere = pl.BlockSpec(memory_space=pltpu.HBM)
    return pl.pallas_call(
        body,
        out_shape=(
            pltpu.VMEM((few, width), BF16),
            pltpu.VMEM((half, width), BF16),
            pltpu.VMEM((half, width), BF16),
        ),
        in_specs=[pl.BlockSpec(memory_space=pltpu.SMEM), anywhere, whole_vmem(), anywhere, whole_vmem(), anywhere],
        out_specs=(whole_vmem(),) * 3,
        scratch_shapes=[
            *(pltpu.VMEM((width, n), BF16) for n in spans),
            pltpu.VMEM((parts, rows, feats), BF16),
            pltpu.VMEM((parts, rows, feats), BF16),
            pltpu.VMEM((parts, rows, feats), F32),
            pltpu.VMEM((rows, width), BF16),
            pltpu.VMEM((rows, 2 * ff), F32),
            pltpu.SemaphoreType.DMA((parts, 2)),
            pltpu.SemaphoreType.DMA((chunks,)),
        ],
        cost_estimate=pl.CostEstimate(flops=6 * rows * width * ff, bytes_accessed=18 << 20, transcendentals=rows * ff),
        name="mixer",
        compiler_params=pltpu.CompilerParams(vmem_limit_bytes=40 << 20),
    )(in_hbm(place), in_hbm(own), in_vmem(other), in_hbm(blocks), gain.reshape(1, width), in_hbm(ffw))


def from_each(value, axis):
    size = lax.axis_size(axis)
    return [value] + [lax.ppermute(value, axis, [(i, (i + k) % size) for i in range(size)]) for k in range(1, size)]


def on_device(
    tokens,
    u_weight,
    v_weight,
    sg_gain,
    spatial_weight,
    spatial_bias,
    out_weight,
    gain_one,
    gate_weight,
    up_weight,
    down_weight,
    gain_two,
):
    core = lax.axis_index("c")
    chips = lax.axis_size("x")
    parts = chips * lax.axis_size("c")
    rows, feats = tokens.shape
    width = feats * parts
    sg = u_weight.shape[1]
    own_rows = rows // parts

    blocks = sent_to_all(tokens, TP)

    ffw = lax.all_gather(jnp.concatenate([gate_weight, up_weight, down_weight.T], axis=1), "y", axis=0, tiled=True)
    ffw = lax.all_gather(ffw, "z", axis=0, tiled=True)

    out_x = lax.all_gather(out_weight.T, "x", axis=1, tiled=True)
    small = jnp.concatenate([u_weight, v_weight, out_x], axis=1)
    depth = small.shape[0]
    small = lax.all_gather(small, "z", axis=0, tiled=True)
    gates = sent_to_all(small[:, : 2 * sg], "y")
    gates = gates.reshape(gates.shape[0], -1, depth, 2 * sg)
    gates = jnp.swapaxes(gates, 0, 1)
    gates = gates.reshape(width, 2 * sg)
    out_rows = from_each(small[:, 2 * sg :], "y")

    whole = jnp.moveaxis(blocks, 0, 1).reshape(rows, width)

    pre_u = jnp.dot(whole, gates[:, :sg], preferred_element_type=F32)
    pre_v = jnp.dot(whole, gates[:, sg:], preferred_element_type=F32)
    gated = jax.nn.gelu(pre_u)
    valued = jax.nn.gelu(pre_v)
    sums = jnp.stack([jnp.sum(valued, axis=1), jnp.sum(valued * valued, axis=1)])
    gains = jnp.concatenate([gain_one, gain_two]).reshape(-1, rows)
    known = sent_to_all(jnp.concatenate([sums, gains], axis=0), TP)
    gains = known[:, 2:].reshape(parts, 2, feats)
    gain_1 = gains[:, 0].reshape(width)
    gain_2 = gains[:, 1].reshape(width)
    sums = jnp.sum(known[:, :2], axis=0)
    count = sg * parts
    mean = sums[0][:, None] / count
    square = sums[1][:, None] / count
    normed = (valued - mean) * lax.rsqrt(square - mean * mean + EPS) * sg_gain[None, :]
    normed = normed.astype(BF16)

    groups = spatial_weight.shape[0]
    block = spatial_weight.shape[1]
    shaped = normed.reshape(rows // block, block, groups, sg // groups)
    lower = jnp.tril(jnp.ones((block, block), jnp.bool_))
    masked = jnp.where(lower[None], spatial_weight, jnp.zeros_like(spatial_weight))
    mixed = jnp.einsum("gij,njgd->nigd", masked, shaped, preferred_element_type=F32)
    mixed = mixed + spatial_bias.T[None, :, :, None]
    gated_out = (gated * mixed.reshape(rows, sg)).astype(BF16)

    together = sent_to_all(gated_out, "x")
    place = jnp.stack([core, lax.axis_index(TP), lax.axis_index("y")]).astype(jnp.int32)
    own = projected(place, together, out_rows)
    mine, keep, give = mixer(place, own, to_partner(own), blocks, gain_1, ffw, gate_weight.shape[1])
    pair = (keep.astype(F32) + to_partner(give).astype(F32)).astype(BF16)
    pieces = lax.all_to_all(pair.reshape(chips, own_rows, width), "x", 0, 0, tiled=True)
    last = last_norm(pieces, mine, gain_2, parts)
    return lax.all_to_all(last, TP, 0, 0, tiled=True).reshape(rows, feats)


def solution(mesh):
    tp = mesh.shape["tp"]
    finer = Mesh(mesh.devices.reshape(16, 4, tp // 2, 2), ("z", "y", "x", "c"))
    return jax.shard_map(
        on_device,
        mesh=finer,
        in_specs=(
            P(FS, TP),
            P(FS, TP),
            P(FS, TP),
            P(TP),
            P(TP, None, None),
            P(TP, None),
            P(TP, FS),
            P(TP),
            P(FS, TP),
            P(FS, TP),
            P(TP, FS),
            P(TP),
        ),
        out_specs=P(FS, TP),
        check_vma=False,
    )
```

```python
import jax
import jax.numpy as jnp
from jax import lax
from jax.experimental import pallas as pl
from jax.experimental.pallas import tpu as pltpu
from jax.sharding import Mesh
from jax.sharding import PartitionSpec as P

FS = ("z", "y")
TP = ("x", "c")

EPS = 1e-05
ALPHA = 2.0**0.25
BF16 = jnp.bfloat16
F32 = jnp.float32
ACROSS = (((1,), (1,)), ((), ()))


def sent_to_all(value, axis):
    copies = jnp.broadcast_to(value, (lax.axis_size(axis), *value.shape))
    return lax.all_to_all(copies, axis, split_axis=0, concat_axis=0, tiled=True)


def to_partner(value):
    return lax.ppermute(value, "c", [(0, 1), (1, 0)])


def row_norm(vals, gain):
    count = vals.shape[1]
    mean = jnp.sum(vals, axis=1, keepdims=True) / count
    square = jnp.sum(vals * vals, axis=1, keepdims=True) / count
    return (vals - mean) * lax.rsqrt(square - mean * mean + EPS) * gain


def in_vmem(value):
    return pltpu.with_memory_space_constraint(value, pltpu.VMEM)


def in_hbm(value):
    return pltpu.with_memory_space_constraint(value, pltpu.HBM)


def whole_vmem():
    return pl.BlockSpec(memory_space=pltpu.VMEM)


def last_norm(pieces, base, gain, parts):
    peers, rows, width = pieces.shape

    def body(pieces_ref, base_ref, gain_ref, out_ref):
        added = pieces_ref[0].astype(F32)
        for k in range(1, peers):
            added = added + pieces_ref[k].astype(F32)
        vals = ALPHA * base_ref[...].astype(F32) + added.astype(BF16).astype(F32)
        done = row_norm(vals, gain_ref[...]).astype(BF16)
        for k in range(parts):
            out_ref[k] = done[:, k * (width // parts) : (k + 1) * (width // parts)]

    return pl.pallas_call(
        body,
        out_shape=pltpu.VMEM((parts, rows, width // parts), BF16),
        in_specs=[whole_vmem()] * 3,
        out_specs=whole_vmem(),
        name="last_norm",
    )(in_vmem(pieces), in_vmem(base), gain.reshape(1, width))


def projected(place, gated, pieces):
    chips, rows, channels = gated.shape
    peers = len(pieces)
    depth = 32
    zs = pieces[0].shape[0] // chips // depth
    width = zs * peers * depth
    steps = 8
    deep = zs // steps
    span = width // steps
    ahead = 3

    def body(place_ref, gated_ref, *rest):
        pieces = rest[:peers]
        out_ref, weights, left, sems = rest[peers:]
        y = place_ref[2]
        copies = []
        for j in range(steps):
            at_z = pl.ds(j * deep, deep)
            some = []
            for n in range(peers):
                at_y = lax.rem(y + peers - n, peers)
                some.append(pltpu.make_async_copy(pieces[n].at[:, at_z], weights.at[:, at_z, at_y], sems.at[j, n]))
            copies.append(some)
        for some in copies[:ahead]:
            for c in some:
                c.start()
        for k in range(chips):
            left[:, k * channels : (k + 1) * channels] = gated_ref[k]
        for j in range(steps):
            for c in copies[j]:
                c.wait()
            if j + ahead < steps:
                for c in copies[j + ahead]:
                    c.start()
            right = [weights[k, j * deep : (j + 1) * deep].reshape(span, channels) for k in range(chips)]
            right = jnp.concatenate(right, axis=1)
            part = lax.dot_general(left[...], right, ACROSS, preferred_element_type=F32)
            out_ref[:, j * span : (j + 1) * span] = part.astype(BF16)

    given = [p.reshape(chips, zs, depth, channels) for p in pieces]
    anywhere = pl.BlockSpec(memory_space=pl.ANY)
    return pl.pallas_call(
        body,
        out_shape=jax.ShapeDtypeStruct((rows, width), BF16),
        in_specs=[pl.BlockSpec(memory_space=pltpu.SMEM), whole_vmem()] + [anywhere] * peers,
        out_specs=whole_vmem(),
        scratch_shapes=[
            pltpu.VMEM((chips, zs, peers, depth, channels), BF16),
            pltpu.VMEM((rows, chips * channels), BF16),
            pltpu.SemaphoreType.DMA((steps, peers)),
        ],
        cost_estimate=pl.CostEstimate(flops=2 * rows * width * chips * channels, bytes_accessed=6 << 20, transcendentals=0),
        name="projected",
    )(in_hbm(place), in_vmem(gated), *given)


def mixer(place, own, other, blocks, gain, ffw, ff):
    rows, width = own.shape
    parts, _, feats = blocks.shape
    chips = parts // 2
    half = rows // 2
    few = rows // parts
    edges = [0, 384, 768, 1152, 2 * ff, 3 * ff]
    spans = [e - b for b, e in zip(edges, edges[1:])]
    chunks = len(spans)
    ahead = 2
    step = 256

    def body(place_ref, own_ref, other_ref, blocks_ref, gain_ref, ffw_ref, mine_ref, keep_ref, give_ref, *rest):
        weights = rest[:chunks]
        base, low, vals, left, acc, in_sems, sems = rest[chunks:]
        core = place_ref[0]
        me = place_ref[1]
        inputs = []
        for j in range(parts):
            at = pl.ds(j * feats, feats)
            inputs.append(
                [
                    pltpu.make_async_copy(own_ref.at[:, at], low.at[j], in_sems.at[j, 0]),
                    pltpu.make_async_copy(blocks_ref.at[j], base.at[j], in_sems.at[j, 1]),
                ]
            )
            for c in inputs[j]:
                c.start()
        copies = []
        for n in range(chunks):
            at = pl.ds(edges[n], spans[n])
            copies.append(pltpu.make_async_copy(ffw_ref.at[:, at], weights[n], sems.at[n]))
        for c in copies[:ahead]:
            c.start()
        total = jnp.zeros((rows, 1), F32)
        squares = jnp.zeros((rows, 1), F32)
        for j in range(parts):
            for c in inputs[j]:
                c.wait()
            high = other_ref[:, j * feats : (j + 1) * feats]
            mix = (low[j].astype(F32) + high.astype(F32)).astype(BF16)
            these = ALPHA * base[j].astype(F32) + mix.astype(F32)
            vals[j] = these
            total += jnp.sum(these, axis=1, keepdims=True)
            squares += jnp.sum(these * these, axis=1, keepdims=True)
        mean = total / width
        scale = lax.rsqrt(squares / width - mean * mean + EPS)
        for j in range(parts):
            at = slice(j * feats, (j + 1) * feats)
            left[:, at] = ((vals[j] - mean) * scale * gain_ref[:, at]).astype(BF16)
        mine_ref[...] = left[pl.ds(pl.multiple_of(me * few, few), few), :]
        for n in range(chunks - 1):
            copies[n].wait()
            if n + ahead < chunks:
                copies[n + ahead].start()
            acc[:, edges[n] : edges[n + 1]] = jnp.dot(left[...], weights[n][...], preferred_element_type=F32)
        gate = acc[:, :ff]
        hidden = (gate * lax.logistic(gate) * acc[:, ff:]).astype(BF16)
        copies[-1].wait()

        def out(keep_core):
            for b in range(0, width, step):
                done = lax.dot_general(hidden, weights[-1][b : b + step], ACROSS, preferred_element_type=F32).astype(BF16)
                for x in range(chips):
                    here = slice(x * few, (x + 1) * few)
                    keep = (2 * x + keep_core) * few
                    give = (2 * x + 1 - keep_core) * few
                    keep_ref[here, b : b + step] = done[keep : keep + few]
                    give_ref[here, b : b + step] = done[give : give + few]

        @pl.when(core == 0)
        def _():
            out(0)

        @pl.when(core == 1)
        def _():
            out(1)

    anywhere = pl.BlockSpec(memory_space=pltpu.HBM)
    return pl.pallas_call(
        body,
        out_shape=(
            pltpu.VMEM((few, width), BF16),
            pltpu.VMEM((half, width), BF16),
            pltpu.VMEM((half, width), BF16),
        ),
        in_specs=[pl.BlockSpec(memory_space=pltpu.SMEM), anywhere, whole_vmem(), anywhere, whole_vmem(), anywhere],
        out_specs=(whole_vmem(),) * 3,
        scratch_shapes=[
            *(pltpu.VMEM((width, n), BF16) for n in spans),
            pltpu.VMEM((parts, rows, feats), BF16),
            pltpu.VMEM((parts, rows, feats), BF16),
            pltpu.VMEM((parts, rows, feats), F32),
            pltpu.VMEM((rows, width), BF16),
            pltpu.VMEM((rows, 2 * ff), F32),
            pltpu.SemaphoreType.DMA((parts, 2)),
            pltpu.SemaphoreType.DMA((chunks,)),
        ],
        cost_estimate=pl.CostEstimate(flops=6 * rows * width * ff, bytes_accessed=18 << 20, transcendentals=rows * ff),
        name="mixer",
        compiler_params=pltpu.CompilerParams(vmem_limit_bytes=40 << 20),
    )(in_hbm(place), in_hbm(own), in_vmem(other), in_hbm(blocks), gain.reshape(1, width), in_hbm(ffw))


def from_each(value, axis):
    size = lax.axis_size(axis)
    return [value] + [lax.ppermute(value, axis, [(i, (i + k) % size) for i in range(size)]) for k in range(1, size)]


def on_device(
    tokens,
    u_weight,
    v_weight,
    sg_gain,
    spatial_weight,
    spatial_bias,
    out_weight,
    gain_one,
    gate_weight,
    up_weight,
    down_weight,
    gain_two,
):
    core = lax.axis_index("c")
    chips = lax.axis_size("x")
    parts = chips * lax.axis_size("c")
    rows, feats = tokens.shape
    width = feats * parts
    sg = u_weight.shape[1]
    own_rows = rows // parts

    blocks = sent_to_all(tokens, TP)

    ffw = lax.all_gather(jnp.concatenate([gate_weight, up_weight, down_weight.T], axis=1), "y", axis=0, tiled=True)
    ffw = lax.all_gather(ffw, "z", axis=0, tiled=True)

    small = jnp.concatenate([u_weight, v_weight, out_weight.T], axis=1)
    depth = small.shape[0]
    small = lax.all_gather(small, "z", axis=0, tiled=True)
    gates = sent_to_all(small[:, : 2 * sg], "y")
    gates = gates.reshape(gates.shape[0], -1, depth, 2 * sg)
    gates = jnp.swapaxes(gates, 0, 1).reshape(width, 2 * sg)
    out_x = lax.all_gather(small[:, 2 * sg :], "x", axis=0, tiled=True)
    out_rows = from_each(out_x, "y")

    whole = jnp.moveaxis(blocks, 0, 1).reshape(rows, width)

    pre_u = jnp.dot(whole, gates[:, :sg], preferred_element_type=F32)
    pre_v = jnp.dot(whole, gates[:, sg:], preferred_element_type=F32)
    gated = jax.nn.gelu(pre_u)
    valued = jax.nn.gelu(pre_v)
    sums = jnp.stack([jnp.sum(valued, axis=1), jnp.sum(valued * valued, axis=1)])
    gains = jnp.concatenate([gain_one, gain_two]).reshape(-1, rows)
    known = sent_to_all(jnp.concatenate([sums, gains], axis=0), TP)
    gains = known[:, 2:].reshape(parts, 2, feats)
    gain_1 = gains[:, 0].reshape(width)
    gain_2 = gains[:, 1].reshape(width)
    sums = jnp.sum(known[:, :2], axis=0)
    count = sg * parts
    mean = sums[0][:, None] / count
    square = sums[1][:, None] / count
    normed = (valued - mean) * lax.rsqrt(square - mean * mean + EPS) * sg_gain[None, :]
    normed = normed.astype(BF16)

    groups = spatial_weight.shape[0]
    block = spatial_weight.shape[1]
    shaped = normed.reshape(rows // block, block, groups, sg // groups)
    lower = jnp.tril(jnp.ones((block, block), jnp.bool_))
    masked = jnp.where(lower[None], spatial_weight, jnp.zeros_like(spatial_weight))
    mixed = jnp.einsum("gij,njgd->nigd", masked, shaped, preferred_element_type=F32)
    mixed = mixed + spatial_bias.T[None, :, :, None]
    gated_out = (gated * mixed.reshape(rows, sg)).astype(BF16)

    together = sent_to_all(gated_out, "x")
    place = jnp.stack([core, lax.axis_index(TP), lax.axis_index("y")]).astype(jnp.int32)
    own = projected(place, together, out_rows)
    mine, keep, give = mixer(place, own, to_partner(own), blocks, gain_1, ffw, gate_weight.shape[1])
    pair = (keep.astype(F32) + to_partner(give).astype(F32)).astype(BF16)
    pieces = lax.all_to_all(pair.reshape(chips, own_rows, width), "x", 0, 0, tiled=True)
    last = last_norm(pieces, mine, gain_2, parts)
    return lax.all_to_all(last, TP, 0, 0, tiled=True).reshape(rows, feats)


def solution(mesh):
    tp = mesh.shape["tp"]
    finer = Mesh(mesh.devices.reshape(16, 4, tp // 2, 2), ("z", "y", "x", "c"))
    return jax.shard_map(
        on_device,
        mesh=finer,
        in_specs=(
            P(FS, TP),
            P(FS, TP),
            P(FS, TP),
            P(TP),
            P(TP, None, None),
            P(TP, None),
            P(TP, FS),
            P(TP),
            P(FS, TP),
            P(FS, TP),
            P(TP, FS),
            P(TP),
        ),
        out_specs=P(FS, TP),
        check_vma=False,
    )
```

```python
import jax
import jax.numpy as jnp
from jax import lax
from jax.experimental import pallas as pl
from jax.experimental.pallas import tpu as pltpu
from jax.sharding import Mesh
from jax.sharding import PartitionSpec as P

FS = ("z", "y")
TP = ("x", "c")

EPS = 1e-05
ALPHA = 2.0**0.25
BF16 = jnp.bfloat16
F32 = jnp.float32
ACROSS = (((1,), (1,)), ((), ()))


def sent_to_all(value, axis):
    copies = jnp.broadcast_to(value, (lax.axis_size(axis), *value.shape))
    return lax.all_to_all(copies, axis, split_axis=0, concat_axis=0, tiled=True)


def to_partner(value):
    return lax.ppermute(value, "c", [(0, 1), (1, 0)])


def row_norm(vals, gain):
    count = vals.shape[1]
    mean = jnp.sum(vals, axis=1, keepdims=True) / count
    square = jnp.sum(vals * vals, axis=1, keepdims=True) / count
    return (vals - mean) * lax.rsqrt(square - mean * mean + EPS) * gain


def in_vmem(value):
    return pltpu.with_memory_space_constraint(value, pltpu.VMEM)


def in_hbm(value):
    return pltpu.with_memory_space_constraint(value, pltpu.HBM)


def whole_vmem():
    return pl.BlockSpec(memory_space=pltpu.VMEM)


def last_norm(pieces, base, gain, parts):
    peers, rows, width = pieces.shape

    def body(pieces_ref, base_ref, gain_ref, out_ref):
        added = pieces_ref[0].astype(F32)
        for k in range(1, peers):
            added = added + pieces_ref[k].astype(F32)
        vals = ALPHA * base_ref[...].astype(F32) + added.astype(BF16).astype(F32)
        done = row_norm(vals, gain_ref[...]).astype(BF16)
        for k in range(parts):
            out_ref[k] = done[:, k * (width // parts) : (k + 1) * (width // parts)]

    return pl.pallas_call(
        body,
        out_shape=pltpu.VMEM((parts, rows, width // parts), BF16),
        in_specs=[whole_vmem()] * 3,
        out_specs=whole_vmem(),
        name="last_norm",
    )(in_vmem(pieces), in_vmem(base), gain.reshape(1, width))


def branches(blocks, gates, gains):
    parts, rows, feats = blocks.shape
    ys, deep, columns = gates.shape
    width = parts * feats
    half = columns // 2
    depth = 32

    def body(blocks_ref, gates_ref, gains_ref, gated_ref, valued_ref, sums_ref, left, right, sems):
        copies = []
        for k in range(parts):
            copies.append(pltpu.make_async_copy(blocks_ref.at[k], left.at[:, pl.ds(k * feats, feats)], sems.at[k]))
            copies[k].start()
        for z in range(deep // depth):
            for y in range(ys):
                at = (z * ys + y) * depth
                right[at : at + depth] = gates_ref[y, z * depth : (z + 1) * depth]
        for c in copies:
            c.wait()
        both = jnp.dot(left[...], right[...], preferred_element_type=F32)
        gated_ref[...] = jax.nn.gelu(both[:, :half])
        valued = jax.nn.gelu(both[:, half:])
        valued_ref[...] = valued
        turned = valued.T
        total = jnp.sum(turned, axis=0, keepdims=True)
        squares = jnp.sum(turned * turned, axis=0, keepdims=True)
        for k in range(parts):
            sums_ref[k, 0:1] = total
            sums_ref[k, 1:2] = squares
            sums_ref[k, 2:3] = gains_ref[...]
            sums_ref[k, 3:4] = gains_ref[...]

    return pl.pallas_call(
        body,
        out_shape=(
            pltpu.VMEM((rows, half), F32),
            pltpu.VMEM((rows, half), F32),
            pltpu.VMEM((parts, 4, rows), F32),
        ),
        in_specs=[pl.BlockSpec(memory_space=pltpu.HBM), whole_vmem(), whole_vmem()],
        out_specs=(whole_vmem(),) * 3,
        scratch_shapes=[
            pltpu.VMEM((rows, width), BF16),
            pltpu.VMEM((width, columns), BF16),
            pltpu.SemaphoreType.DMA((parts,)),
        ],
        compiler_params=pltpu.CompilerParams(vmem_limit_bytes=24 << 20),
        cost_estimate=pl.CostEstimate(flops=2 * rows * width * columns, bytes_accessed=4 << 20, transcendentals=2 * rows * columns),
        name="branches",
    )(in_hbm(blocks), in_vmem(gates), gains)


def gated_copies(known, gated, valued, gain, weight, bias, copies):
    parts, _, rows = known.shape
    channels = gated.shape[1]
    block = weight.shape[1]
    count = parts * channels

    def body(known_ref, gated_ref, valued_ref, gain_ref, weight_ref, bias_ref, out_ref):
        sums = known_ref[0]
        for k in range(1, parts):
            sums = sums + known_ref[k]
        mean = sums[0:1] / count
        square = sums[1:2] / count
        scale = lax.rsqrt(square - mean * mean + EPS)
        mean = jnp.broadcast_to(mean, (channels, rows)).T
        scale = jnp.broadcast_to(scale, (channels, rows)).T
        normed = ((valued_ref[...] - mean) * scale * gain_ref[...]).astype(BF16)
        row = lax.broadcasted_iota(jnp.int32, (block, block), 0)
        column = lax.broadcasted_iota(jnp.int32, (block, block), 1)
        masked = jnp.where(row >= column, weight_ref[0].astype(F32), 0.0).astype(BF16)
        offset = jnp.broadcast_to(bias_ref[...], (channels, block)).T
        for n in range(rows // block):
            at = slice(n * block, (n + 1) * block)
            mixed = jnp.dot(masked, normed[at], preferred_element_type=F32) + offset
            done = (gated_ref[at] * mixed).astype(BF16)
            for k in range(copies):
                out_ref[k, at] = done

    return pl.pallas_call(
        body,
        out_shape=pltpu.VMEM((copies, rows, channels), BF16),
        in_specs=[whole_vmem()] * 6,
        out_specs=whole_vmem(),
        compiler_params=pltpu.CompilerParams(vmem_limit_bytes=12 << 20),
        cost_estimate=pl.CostEstimate(flops=2 * rows * block * channels, bytes_accessed=2 << 20, transcendentals=rows),
        name="gated_copies",
    )(in_vmem(known), in_vmem(gated), in_vmem(valued), gain.reshape(1, channels), weight, bias)


def projected(place, gated, pieces):
    chips, rows, channels = gated.shape
    peers = len(pieces)
    depth = 32
    zs = pieces[0].shape[0] // chips // depth
    width = zs * peers * depth
    steps = 8
    deep = zs // steps
    span = width // steps
    ahead = 3

    def body(place_ref, gated_ref, *rest):
        pieces = rest[:peers]
        out_ref, weights, left, sems = rest[peers:]
        y = place_ref[2]
        copies = []
        for j in range(steps):
            at_z = pl.ds(j * deep, deep)
            some = []
            for n in range(peers):
                at_y = lax.rem(y + peers - n, peers)
                some.append(pltpu.make_async_copy(pieces[n].at[:, at_z], weights.at[:, at_z, at_y], sems.at[j, n]))
            copies.append(some)
        for some in copies[:ahead]:
            for c in some:
                c.start()
        for k in range(chips):
            left[:, k * channels : (k + 1) * channels] = gated_ref[k]
        for j in range(steps):
            for c in copies[j]:
                c.wait()
            if j + ahead < steps:
                for c in copies[j + ahead]:
                    c.start()
            right = [weights[k, j * deep : (j + 1) * deep].reshape(span, channels) for k in range(chips)]
            right = jnp.concatenate(right, axis=1)
            part = lax.dot_general(left[...], right, ACROSS, preferred_element_type=F32)
            out_ref[:, j * span : (j + 1) * span] = part.astype(BF16)

    given = [p.reshape(chips, zs, depth, channels) for p in pieces]
    anywhere = pl.BlockSpec(memory_space=pl.ANY)
    return pl.pallas_call(
        body,
        out_shape=jax.ShapeDtypeStruct((rows, width), BF16),
        in_specs=[pl.BlockSpec(memory_space=pltpu.SMEM), whole_vmem()] + [anywhere] * peers,
        out_specs=whole_vmem(),
        scratch_shapes=[
            pltpu.VMEM((chips, zs, peers, depth, channels), BF16),
            pltpu.VMEM((rows, chips * channels), BF16),
            pltpu.SemaphoreType.DMA((steps, peers)),
        ],
        cost_estimate=pl.CostEstimate(flops=2 * rows * width * chips * channels, bytes_accessed=6 << 20, transcendentals=0),
        name="projected",
    )(in_hbm(place), in_vmem(gated), *given)


def mixer(place, own, other, blocks, gain, ffw, ff):
    rows, width = own.shape
    parts, _, feats = blocks.shape
    chips = parts // 2
    half = rows // 2
    few = rows // parts
    edges = [0, 384, 768, 1152, 2 * ff, 3 * ff]
    spans = [e - b for b, e in zip(edges, edges[1:])]
    chunks = len(spans)
    ahead = 3
    step = 256

    def body(place_ref, own_ref, other_ref, blocks_ref, gain_ref, ffw_ref, mine_ref, keep_ref, give_ref, *rest):
        weights = rest[:chunks]
        base, low, vals, left, acc, in_sems, sems = rest[chunks:]
        core = place_ref[0]
        me = place_ref[1]
        inputs = []
        for j in range(parts):
            at = pl.ds(j * feats, feats)
            inputs.append(
                [
                    pltpu.make_async_copy(own_ref.at[:, at], low.at[j], in_sems.at[j, 0]),
                    pltpu.make_async_copy(blocks_ref.at[j], base.at[j], in_sems.at[j, 1]),
                ]
            )
            for c in inputs[j]:
                c.start()
        copies = []
        for n in range(chunks):
            at = pl.ds(edges[n], spans[n])
            copies.append(pltpu.make_async_copy(ffw_ref.at[:, at], weights[n], sems.at[n]))
        for c in copies[:ahead]:
            c.start()
        total = jnp.zeros((rows, 1), F32)
        squares = jnp.zeros((rows, 1), F32)
        for j in range(parts):
            for c in inputs[j]:
                c.wait()
            high = other_ref[:, j * feats : (j + 1) * feats]
            mix = (low[j].astype(F32) + high.astype(F32)).astype(BF16)
            these = ALPHA * base[j].astype(F32) + mix.astype(F32)
            vals[j] = these
            total += jnp.sum(these, axis=1, keepdims=True)
            squares += jnp.sum(these * these, axis=1, keepdims=True)
        mean = total / width
        scale = lax.rsqrt(squares / width - mean * mean + EPS)
        for j in range(parts):
            at = slice(j * feats, (j + 1) * feats)
            left[:, at] = ((vals[j] - mean) * scale * gain_ref[:, at]).astype(BF16)
        mine_ref[...] = left[pl.ds(pl.multiple_of(me * few, few), few), :]
        for n in range(chunks - 1):
            copies[n].wait()
            if n + ahead < chunks:
                copies[n + ahead].start()
            acc[:, edges[n] : edges[n + 1]] = jnp.dot(left[...], weights[n][...], preferred_element_type=F32)
        gate = acc[:, :ff]
        hidden = (gate * lax.logistic(gate) * acc[:, ff:]).astype(BF16)
        copies[-1].wait()

        def out(keep_core):
            for b in range(0, width, step):
                done = lax.dot_general(hidden, weights[-1][b : b + step], ACROSS, preferred_element_type=F32).astype(BF16)
                for x in range(chips):
                    here = slice(x * few, (x + 1) * few)
                    keep = (2 * x + keep_core) * few
                    give = (2 * x + 1 - keep_core) * few
                    keep_ref[here, b : b + step] = done[keep : keep + few]
                    give_ref[here, b : b + step] = done[give : give + few]

        @pl.when(core == 0)
        def _():
            out(0)

        @pl.when(core == 1)
        def _():
            out(1)

    anywhere = pl.BlockSpec(memory_space=pltpu.HBM)
    return pl.pallas_call(
        body,
        out_shape=(
            pltpu.VMEM((few, width), BF16),
            pltpu.VMEM((half, width), BF16),
            pltpu.VMEM((half, width), BF16),
        ),
        in_specs=[pl.BlockSpec(memory_space=pltpu.SMEM), anywhere, whole_vmem(), anywhere, whole_vmem(), anywhere],
        out_specs=(whole_vmem(),) * 3,
        scratch_shapes=[
            *(pltpu.VMEM((width, n), BF16) for n in spans),
            pltpu.VMEM((parts, rows, feats), BF16),
            pltpu.VMEM((parts, rows, feats), BF16),
            pltpu.VMEM((parts, rows, feats), F32),
            pltpu.VMEM((rows, width), BF16),
            pltpu.VMEM((rows, 2 * ff), F32),
            pltpu.SemaphoreType.DMA((parts, 2)),
            pltpu.SemaphoreType.DMA((chunks,)),
        ],
        cost_estimate=pl.CostEstimate(flops=6 * rows * width * ff, bytes_accessed=18 << 20, transcendentals=rows * ff),
        name="mixer",
        compiler_params=pltpu.CompilerParams(vmem_limit_bytes=40 << 20),
    )(in_hbm(place), in_hbm(own), in_vmem(other), in_hbm(blocks), gain.reshape(1, width), in_hbm(ffw))


def from_each(value, axis):
    size = lax.axis_size(axis)
    return [value] + [lax.ppermute(value, axis, [(i, (i + k) % size) for i in range(size)]) for k in range(1, size)]


def on_device(
    tokens,
    u_weight,
    v_weight,
    sg_gain,
    spatial_weight,
    spatial_bias,
    out_weight,
    gain_one,
    gate_weight,
    up_weight,
    down_weight,
    gain_two,
):
    core = lax.axis_index("c")
    chips = lax.axis_size("x")
    parts = chips * lax.axis_size("c")
    rows, feats = tokens.shape
    width = feats * parts
    sg = u_weight.shape[1]
    own_rows = rows // parts

    blocks = sent_to_all(tokens, TP)

    ffw = lax.all_gather(jnp.concatenate([gate_weight, up_weight, down_weight.T], axis=1), "y", axis=0, tiled=True)
    ffw = lax.all_gather(ffw, "z", axis=0, tiled=True)

    small = jnp.concatenate([u_weight, v_weight, out_weight.T], axis=1)
    small = lax.all_gather(small, "z", axis=0, tiled=True)
    gates = sent_to_all(small[:, : 2 * sg], "y")
    out_x = lax.all_gather(small[:, 2 * sg :], "x", axis=0, tiled=True)
    out_rows = from_each(out_x, "y")

    gains = jnp.concatenate([gain_one, gain_two]).reshape(1, rows)
    gated, valued, sums = branches(blocks, gates, gains)
    known = lax.all_to_all(sums, TP, 0, 0, tiled=True)
    gains = known[:, 2].reshape(parts, 2, feats)
    gain_1 = gains[:, 0].reshape(width)
    gain_2 = gains[:, 1].reshape(width)
    copies = gated_copies(known, gated, valued, sg_gain, spatial_weight, spatial_bias, chips)
    together = lax.all_to_all(copies, "x", 0, 0, tiled=True)
    place = jnp.stack([core, lax.axis_index(TP), lax.axis_index("y")]).astype(jnp.int32)
    own = projected(place, together, out_rows)
    mine, keep, give = mixer(place, own, to_partner(own), blocks, gain_1, ffw, gate_weight.shape[1])
    pair = (keep.astype(F32) + to_partner(give).astype(F32)).astype(BF16)
    pieces = lax.all_to_all(pair.reshape(chips, own_rows, width), "x", 0, 0, tiled=True)
    last = last_norm(pieces, mine, gain_2, parts)
    return lax.all_to_all(last, TP, 0, 0, tiled=True).reshape(rows, feats)


def solution(mesh):
    tp = mesh.shape["tp"]
    finer = Mesh(mesh.devices.reshape(16, 4, tp // 2, 2), ("z", "y", "x", "c"))
    return jax.shard_map(
        on_device,
        mesh=finer,
        in_specs=(
            P(FS, TP),
            P(FS, TP),
            P(FS, TP),
            P(TP),
            P(TP, None, None),
            P(TP, None),
            P(TP, FS),
            P(TP),
            P(FS, TP),
            P(FS, TP),
            P(TP, FS),
            P(TP),
        ),
        out_specs=P(FS, TP),
        check_vma=False,
    )
```

```python
import jax
import jax.numpy as jnp
from jax import lax
from jax.experimental import pallas as pl
from jax.experimental.pallas import tpu as pltpu
from jax.sharding import Mesh
from jax.sharding import PartitionSpec as P

FS = ("z", "y")
TP = ("x", "c")

EPS = 1e-05
ALPHA = 2.0**0.25
BF16 = jnp.bfloat16
F32 = jnp.float32
ACROSS = (((1,), (1,)), ((), ()))


def sent_to_all(value, axis):
    copies = jnp.broadcast_to(value, (lax.axis_size(axis), *value.shape))
    return lax.all_to_all(copies, axis, split_axis=0, concat_axis=0, tiled=True)


def to_partner(value):
    return lax.ppermute(value, "c", [(0, 1), (1, 0)])


def row_norm(vals, gain):
    count = vals.shape[1]
    mean = jnp.sum(vals, axis=1, keepdims=True) / count
    square = jnp.sum(vals * vals, axis=1, keepdims=True) / count
    return (vals - mean) * lax.rsqrt(square - mean * mean + EPS) * gain


def in_vmem(value):
    return pltpu.with_memory_space_constraint(value, pltpu.VMEM)


def in_hbm(value):
    return pltpu.with_memory_space_constraint(value, pltpu.HBM)


def whole_vmem():
    return pl.BlockSpec(memory_space=pltpu.VMEM)


def last_norm(pieces, base, gain, parts):
    peers, rows, width = pieces.shape

    def body(pieces_ref, base_ref, gain_ref, out_ref):
        added = pieces_ref[0].astype(F32)
        for k in range(1, peers):
            added = added + pieces_ref[k].astype(F32)
        vals = ALPHA * base_ref[...].astype(F32) + added.astype(BF16).astype(F32)
        done = row_norm(vals, gain_ref[...]).astype(BF16)
        for k in range(parts):
            out_ref[k] = done[:, k * (width // parts) : (k + 1) * (width // parts)]

    return pl.pallas_call(
        body,
        out_shape=pltpu.VMEM((parts, rows, width // parts), BF16),
        in_specs=[whole_vmem()] * 3,
        out_specs=whole_vmem(),
        name="last_norm",
    )(in_vmem(pieces), in_vmem(base), gain.reshape(1, width))


def branches(blocks, gates, gains):
    parts, rows, feats = blocks.shape
    ys, deep, columns = gates.shape
    width = parts * feats
    half = columns // 2
    depth = 32

    def body(blocks_ref, gates_ref, gains_ref, gated_ref, valued_ref, sums_ref, left, right, sems):
        copies = []
        for k in range(parts):
            copies.append(pltpu.make_async_copy(blocks_ref.at[k], left.at[:, pl.ds(k * feats, feats)], sems.at[k]))
            copies[k].start()
        for z in range(deep // depth):
            for y in range(ys):
                at = (z * ys + y) * depth
                right[at : at + depth] = gates_ref[y, z * depth : (z + 1) * depth]
        for c in copies:
            c.wait()
        both = jnp.dot(left[...], right[...], preferred_element_type=F32)
        gated_ref[...] = jax.nn.gelu(both[:, :half])
        valued = jax.nn.gelu(both[:, half:])
        valued_ref[...] = valued
        turned = valued.T
        total = jnp.sum(turned, axis=0, keepdims=True)
        squares = jnp.sum(turned * turned, axis=0, keepdims=True)
        for k in range(parts):
            sums_ref[k, 0:1] = total
            sums_ref[k, 1:2] = squares
            sums_ref[k, 2:3] = gains_ref[...]
            sums_ref[k, 3:4] = gains_ref[...]

    return pl.pallas_call(
        body,
        out_shape=(
            pltpu.VMEM((rows, half), F32),
            pltpu.VMEM((rows, half), F32),
            pltpu.VMEM((parts, 4, rows), F32),
        ),
        in_specs=[pl.BlockSpec(memory_space=pltpu.HBM), whole_vmem(), whole_vmem()],
        out_specs=(whole_vmem(),) * 3,
        scratch_shapes=[
            pltpu.VMEM((rows, width), BF16),
            pltpu.VMEM((width, columns), BF16),
            pltpu.SemaphoreType.DMA((parts,)),
        ],
        compiler_params=pltpu.CompilerParams(vmem_limit_bytes=24 << 20),
        cost_estimate=pl.CostEstimate(flops=2 * rows * width * columns, bytes_accessed=4 << 20, transcendentals=2 * rows * columns),
        name="branches",
    )(in_hbm(blocks), in_vmem(gates), gains)


def gated_copies(known, gated, valued, gain, weight, bias, copies):
    parts, _, rows = known.shape
    channels = gated.shape[1]
    block = weight.shape[1]
    count = parts * channels

    def body(known_ref, gated_ref, valued_ref, gain_ref, weight_ref, bias_ref, out_ref):
        sums = known_ref[0]
        for k in range(1, parts):
            sums = sums + known_ref[k]
        mean = sums[0:1] / count
        square = sums[1:2] / count
        scale = lax.rsqrt(square - mean * mean + EPS)
        mean = jnp.broadcast_to(mean, (channels, rows)).T
        scale = jnp.broadcast_to(scale, (channels, rows)).T
        normed = ((valued_ref[...] - mean) * scale * gain_ref[...]).astype(BF16)
        row = lax.broadcasted_iota(jnp.int32, (block, block), 0)
        column = lax.broadcasted_iota(jnp.int32, (block, block), 1)
        masked = jnp.where(row >= column, weight_ref[0].astype(F32), 0.0).astype(BF16)
        offset = jnp.broadcast_to(bias_ref[...], (channels, block)).T
        for n in range(rows // block):
            at = slice(n * block, (n + 1) * block)
            mixed = jnp.dot(masked, normed[at], preferred_element_type=F32) + offset
            done = (gated_ref[at] * mixed).astype(BF16)
            for k in range(copies):
                out_ref[k, at] = done

    return pl.pallas_call(
        body,
        out_shape=pltpu.VMEM((copies, rows, channels), BF16),
        in_specs=[whole_vmem()] * 6,
        out_specs=whole_vmem(),
        compiler_params=pltpu.CompilerParams(vmem_limit_bytes=12 << 20),
        cost_estimate=pl.CostEstimate(flops=2 * rows * block * channels, bytes_accessed=2 << 20, transcendentals=rows),
        name="gated_copies",
    )(in_vmem(known), in_vmem(gated), in_vmem(valued), gain.reshape(1, channels), weight, bias)


def projected(place, gated, pieces):
    chips, rows, channels = gated.shape
    peers = len(pieces)
    depth = 32
    zs = pieces[0].shape[0] // chips // depth
    width = zs * peers * depth
    steps = 8
    deep = zs // steps
    span = width // steps
    ahead = 3

    def body(place_ref, gated_ref, *rest):
        pieces = rest[:peers]
        out_ref, weights, left, sems = rest[peers:]
        y = place_ref[2]
        copies = []
        for j in range(steps):
            at_z = pl.ds(j * deep, deep)
            some = []
            for n in range(peers):
                at_y = lax.rem(y + peers - n, peers)
                some.append(pltpu.make_async_copy(pieces[n].at[:, at_z], weights.at[:, at_z, at_y], sems.at[j, n]))
            copies.append(some)
        for some in copies[:ahead]:
            for c in some:
                c.start()
        for k in range(chips):
            left[:, k * channels : (k + 1) * channels] = gated_ref[k]
        for j in range(steps):
            for c in copies[j]:
                c.wait()
            if j + ahead < steps:
                for c in copies[j + ahead]:
                    c.start()
            right = [weights[k, j * deep : (j + 1) * deep].reshape(span, channels) for k in range(chips)]
            right = jnp.concatenate(right, axis=1)
            part = lax.dot_general(left[...], right, ACROSS, preferred_element_type=F32)
            out_ref[:, j * span : (j + 1) * span] = part.astype(BF16)

    given = [p.reshape(chips, zs, depth, channels) for p in pieces]
    anywhere = pl.BlockSpec(memory_space=pl.ANY)
    return pl.pallas_call(
        body,
        out_shape=jax.ShapeDtypeStruct((rows, width), BF16),
        in_specs=[pl.BlockSpec(memory_space=pltpu.SMEM), whole_vmem()] + [anywhere] * peers,
        out_specs=whole_vmem(),
        scratch_shapes=[
            pltpu.VMEM((chips, zs, peers, depth, channels), BF16),
            pltpu.VMEM((rows, chips * channels), BF16),
            pltpu.SemaphoreType.DMA((steps, peers)),
        ],
        cost_estimate=pl.CostEstimate(flops=2 * rows * width * chips * channels, bytes_accessed=6 << 20, transcendentals=0),
        name="projected",
    )(in_hbm(place), in_vmem(gated), *given)


def copies_of(value, count):
    def body(value_ref, out_ref):
        for k in range(count):
            out_ref[k] = value_ref[...]

    return pl.pallas_call(
        body,
        out_shape=pltpu.VMEM((count, *value.shape), value.dtype),
        in_specs=[whole_vmem()],
        out_specs=whole_vmem(),
        compiler_params=pltpu.CompilerParams(vmem_limit_bytes=8 << 20),
        name="copies",
    )(value)


def first_rows(place, own, other, blocks, gain):
    rows, width = own.shape
    parts, _, feats = blocks.shape
    few = rows // parts
    lanes = 128

    def body(place_ref, own_ref, other_ref, blocks_ref, gain_ref, first_ref, mine_ref, base, low, vals, sems):
        me = place_ref[1]
        inputs = []
        for j in range(parts):
            at = pl.ds(j * feats, feats)
            inputs.append(
                [
                    pltpu.make_async_copy(own_ref.at[:, at], low.at[j], sems.at[j, 0]),
                    pltpu.make_async_copy(blocks_ref.at[j], base.at[j], sems.at[j, 1]),
                ]
            )
            for c in inputs[j]:
                c.start()
        total = jnp.zeros((rows, lanes), F32)
        squares = jnp.zeros((rows, lanes), F32)
        for j in range(parts):
            for c in inputs[j]:
                c.wait()
            for b in range(0, feats, lanes):
                at = slice(j * feats + b, j * feats + b + lanes)
                high = other_ref[:, at]
                mix = (low[j, :, b : b + lanes].astype(F32) + high.astype(F32)).astype(BF16)
                these = ALPHA * base[j, :, b : b + lanes].astype(F32) + mix.astype(F32)
                vals[:, at] = these
                total += these
                squares += these * these
        mean = jnp.sum(total, axis=1, keepdims=True) / width
        scale = lax.rsqrt(jnp.sum(squares, axis=1, keepdims=True) / width - mean * mean + EPS)
        for j in range(parts):
            at = slice(j * feats, (j + 1) * feats)
            first_ref[:, at] = ((vals[:, at] - mean) * scale * gain_ref[:, at]).astype(BF16)
        mine_ref[...] = first_ref[pl.ds(pl.multiple_of(me * few, few), few), :]

    hbm = pl.BlockSpec(memory_space=pltpu.HBM)
    return pl.pallas_call(
        body,
        out_shape=(jax.ShapeDtypeStruct((rows, width), BF16), pltpu.VMEM((few, width), BF16)),
        in_specs=[pl.BlockSpec(memory_space=pltpu.SMEM), hbm, whole_vmem(), hbm, whole_vmem()],
        out_specs=(whole_vmem(),) * 2,
        scratch_shapes=[
            pltpu.VMEM((parts, rows, feats), BF16),
            pltpu.VMEM((parts, rows, feats), BF16),
            pltpu.VMEM((rows, width), F32),
            pltpu.SemaphoreType.DMA((parts, 2)),
        ],
        compiler_params=pltpu.CompilerParams(vmem_limit_bytes=16 << 20),
        cost_estimate=pl.CostEstimate(flops=12 * rows * width, bytes_accessed=6 << 20, transcendentals=rows),
        name="first_rows",
    )(in_hbm(place), in_hbm(own), in_vmem(other), in_hbm(blocks), gain.reshape(1, width))


def mixer(place, first, ffw, ff):
    rows, width = first.shape
    chips = 4
    half = rows // 2
    few = half // chips
    edges = [0, 384, 768, 1152, 2 * ff, 3 * ff]
    spans = [e - b for b, e in zip(edges, edges[1:])]
    chunks = len(spans)
    ahead = 3
    step = 256

    def body(place_ref, first_ref, ffw_ref, keep_ref, give_ref, *rest):
        weights = rest[:chunks]
        left, acc, lead, sems = rest[chunks:]
        core = place_ref[0]
        start = pltpu.make_async_copy(first_ref, left, lead.at[0])
        start.start()
        copies = []
        for n in range(chunks):
            at = pl.ds(edges[n], spans[n])
            copies.append(pltpu.make_async_copy(ffw_ref.at[:, at], weights[n], sems.at[n]))
        for c in copies[:ahead]:
            c.start()
        start.wait()
        for n in range(chunks - 1):
            copies[n].wait()
            if n + ahead < chunks:
                copies[n + ahead].start()
            acc[:, edges[n] : edges[n + 1]] = jnp.dot(left[...], weights[n][...], preferred_element_type=F32)
        gate = acc[:, :ff]
        hidden = (gate * lax.logistic(gate) * acc[:, ff:]).astype(BF16)
        copies[-1].wait()

        def out(keep_core):
            for b in range(0, width, step):
                done = lax.dot_general(hidden, weights[-1][b : b + step], ACROSS, preferred_element_type=F32).astype(BF16)
                for x in range(chips):
                    here = slice(x * few, (x + 1) * few)
                    keep = (2 * x + keep_core) * few
                    give = (2 * x + 1 - keep_core) * few
                    keep_ref[here, b : b + step] = done[keep : keep + few]
                    give_ref[here, b : b + step] = done[give : give + few]

        @pl.when(core == 0)
        def _():
            out(0)

        @pl.when(core == 1)
        def _():
            out(1)

    return pl.pallas_call(
        body,
        out_shape=(
            pltpu.VMEM((half, width), BF16),
            pltpu.VMEM((half, width), BF16),
        ),
        in_specs=[pl.BlockSpec(memory_space=pltpu.SMEM)] + [pl.BlockSpec(memory_space=pltpu.HBM)] * 2,
        out_specs=(whole_vmem(),) * 2,
        scratch_shapes=[
            *(pltpu.VMEM((width, n), BF16) for n in spans),
            pltpu.VMEM((rows, width), BF16),
            pltpu.VMEM((rows, 2 * ff), F32),
            pltpu.SemaphoreType.DMA((1,)),
            pltpu.SemaphoreType.DMA((chunks,)),
        ],
        cost_estimate=pl.CostEstimate(flops=6 * rows * width * ff, bytes_accessed=18 << 20, transcendentals=rows * ff),
        name="mixer",
        compiler_params=pltpu.CompilerParams(vmem_limit_bytes=28 << 20),
    )(in_hbm(place), in_hbm(first), in_hbm(ffw))


def from_each(value, axis):
    size = lax.axis_size(axis)
    return [value] + [lax.ppermute(value, axis, [(i, (i + k) % size) for i in range(size)]) for k in range(1, size)]


def on_device(
    tokens,
    u_weight,
    v_weight,
    sg_gain,
    spatial_weight,
    spatial_bias,
    out_weight,
    gain_one,
    gate_weight,
    up_weight,
    down_weight,
    gain_two,
):
    core = lax.axis_index("c")
    chips = lax.axis_size("x")
    parts = chips * lax.axis_size("c")
    rows, feats = tokens.shape
    width = feats * parts
    sg = u_weight.shape[1]
    own_rows = rows // parts

    blocks = lax.all_to_all(copies_of(tokens, parts), TP, 0, 0, tiled=True)

    ffw = lax.all_gather(jnp.concatenate([gate_weight, up_weight, down_weight.T], axis=1), "y", axis=0, tiled=True)
    ffw = lax.all_gather(ffw, "z", axis=0, tiled=True)

    small = jnp.concatenate([u_weight, v_weight, out_weight.T], axis=1)
    small = lax.all_gather(small, "z", axis=0, tiled=True)
    gates = sent_to_all(small[:, : 2 * sg], "y")
    out_x = lax.all_gather(small[:, 2 * sg :], "x", axis=0, tiled=True)
    out_rows = from_each(out_x, "y")

    gains = jnp.concatenate([gain_one, gain_two]).reshape(1, rows)
    gated, valued, sums = branches(blocks, gates, gains)
    known = lax.all_to_all(sums, TP, 0, 0, tiled=True)
    gains = known[:, 2].reshape(parts, 2, feats)
    gain_1 = gains[:, 0].reshape(width)
    gain_2 = gains[:, 1].reshape(width)
    copies = gated_copies(known, gated, valued, sg_gain, spatial_weight, spatial_bias, chips)
    together = lax.all_to_all(copies, "x", 0, 0, tiled=True)
    place = jnp.stack([core, lax.axis_index(TP), lax.axis_index("y")]).astype(jnp.int32)
    own = projected(place, together, out_rows)
    first, mine = first_rows(place, own, to_partner(own), blocks, gain_1)
    keep, give = mixer(place, first, ffw, gate_weight.shape[1])
    pair = (keep.astype(F32) + to_partner(give).astype(F32)).astype(BF16)
    pieces = lax.all_to_all(pair.reshape(chips, own_rows, width), "x", 0, 0, tiled=True)
    last = last_norm(pieces, mine, gain_2, parts)
    return lax.all_to_all(last, TP, 0, 0, tiled=True).reshape(rows, feats)


def solution(mesh):
    tp = mesh.shape["tp"]
    finer = Mesh(mesh.devices.reshape(16, 4, tp // 2, 2), ("z", "y", "x", "c"))
    return jax.shard_map(
        on_device,
        mesh=finer,
        in_specs=(
            P(FS, TP),
            P(FS, TP),
            P(FS, TP),
            P(TP),
            P(TP, None, None),
            P(TP, None),
            P(TP, FS),
            P(TP),
            P(FS, TP),
            P(FS, TP),
            P(TP, FS),
            P(TP),
        ),
        out_specs=P(FS, TP),
        check_vma=False,
    )
```

```python
import jax
import jax.numpy as jnp
from jax import lax
from jax.experimental import pallas as pl
from jax.experimental.pallas import tpu as pltpu
from jax.sharding import Mesh
from jax.sharding import PartitionSpec as P

FS = ("z", "y")
TP = ("x", "c")

EPS = 1e-05
ALPHA = 2.0**0.25
BF16 = jnp.bfloat16
F32 = jnp.float32
ACROSS = (((1,), (1,)), ((), ()))


def sent_to_all(value, axis):
    copies = jnp.broadcast_to(value, (lax.axis_size(axis), *value.shape))
    return lax.all_to_all(copies, axis, split_axis=0, concat_axis=0, tiled=True)


def to_partner(value):
    return lax.ppermute(value, "c", [(0, 1), (1, 0)])


def row_norm(vals, gain):
    count = vals.shape[1]
    mean = jnp.sum(vals, axis=1, keepdims=True) / count
    square = jnp.sum(vals * vals, axis=1, keepdims=True) / count
    return (vals - mean) * lax.rsqrt(square - mean * mean + EPS) * gain


def in_vmem(value):
    return pltpu.with_memory_space_constraint(value, pltpu.VMEM)


def in_hbm(value):
    return pltpu.with_memory_space_constraint(value, pltpu.HBM)


def whole_vmem():
    return pl.BlockSpec(memory_space=pltpu.VMEM)


def last_norm(pieces, base, gain, parts):
    peers, rows, width = pieces.shape

    def body(pieces_ref, base_ref, gain_ref, out_ref):
        added = pieces_ref[0].astype(F32)
        for k in range(1, peers):
            added = added + pieces_ref[k].astype(F32)
        vals = ALPHA * base_ref[...].astype(F32) + added.astype(BF16).astype(F32)
        done = row_norm(vals, gain_ref[...]).astype(BF16)
        for k in range(parts):
            out_ref[k] = done[:, k * (width // parts) : (k + 1) * (width // parts)]

    return pl.pallas_call(
        body,
        out_shape=pltpu.VMEM((parts, rows, width // parts), BF16),
        in_specs=[whole_vmem()] * 3,
        out_specs=whole_vmem(),
        name="last_norm",
    )(in_vmem(pieces), in_vmem(base), gain.reshape(1, width))


def branches(blocks, gates, gains):
    parts, rows, feats = blocks.shape
    ys, deep, columns = gates.shape
    width = parts * feats
    half = columns // 2
    depth = 32

    def body(blocks_ref, gates_ref, gains_ref, gated_ref, valued_ref, sums_ref, left, right, sems):
        copies = []
        for k in range(parts):
            copies.append(pltpu.make_async_copy(blocks_ref.at[k], left.at[:, pl.ds(k * feats, feats)], sems.at[k]))
            copies[k].start()
        for z in range(deep // depth):
            for y in range(ys):
                at = (z * ys + y) * depth
                right[at : at + depth] = gates_ref[y, z * depth : (z + 1) * depth]
        for c in copies:
            c.wait()
        both = jnp.dot(left[...], right[...], preferred_element_type=F32)
        gated_ref[...] = jax.nn.gelu(both[:, :half])
        valued = jax.nn.gelu(both[:, half:])
        valued_ref[...] = valued
        turned = valued.T
        total = jnp.sum(turned, axis=0, keepdims=True)
        squares = jnp.sum(turned * turned, axis=0, keepdims=True)
        for k in range(parts):
            sums_ref[k, 0:1] = total
            sums_ref[k, 1:2] = squares
            sums_ref[k, 2:3] = gains_ref[...]
            sums_ref[k, 3:4] = gains_ref[...]

    return pl.pallas_call(
        body,
        out_shape=(
            pltpu.VMEM((rows, half), F32),
            pltpu.VMEM((rows, half), F32),
            pltpu.VMEM((parts, 4, rows), F32),
        ),
        in_specs=[pl.BlockSpec(memory_space=pltpu.HBM), whole_vmem(), whole_vmem()],
        out_specs=(whole_vmem(),) * 3,
        scratch_shapes=[
            pltpu.VMEM((rows, width), BF16),
            pltpu.VMEM((width, columns), BF16),
            pltpu.SemaphoreType.DMA((parts,)),
        ],
        compiler_params=pltpu.CompilerParams(vmem_limit_bytes=24 << 20),
        cost_estimate=pl.CostEstimate(flops=2 * rows * width * columns, bytes_accessed=4 << 20, transcendentals=2 * rows * columns),
        name="branches",
    )(in_hbm(blocks), in_vmem(gates), gains)


def gated_copies(known, gated, valued, gain, weight, bias, copies):
    parts, _, rows = known.shape
    channels = gated.shape[1]
    block = weight.shape[1]
    count = parts * channels

    def body(known_ref, gated_ref, valued_ref, gain_ref, weight_ref, bias_ref, out_ref):
        sums = known_ref[0]
        for k in range(1, parts):
            sums = sums + known_ref[k]
        mean = sums[0:1] / count
        square = sums[1:2] / count
        scale = lax.rsqrt(square - mean * mean + EPS)
        mean = jnp.broadcast_to(mean, (channels, rows)).T
        scale = jnp.broadcast_to(scale, (channels, rows)).T
        normed = ((valued_ref[...] - mean) * scale * gain_ref[...]).astype(BF16)
        row = lax.broadcasted_iota(jnp.int32, (block, block), 0)
        column = lax.broadcasted_iota(jnp.int32, (block, block), 1)
        masked = jnp.where(row >= column, weight_ref[0].astype(F32), 0.0).astype(BF16)
        offset = jnp.broadcast_to(bias_ref[...], (channels, block)).T
        for n in range(rows // block):
            at = slice(n * block, (n + 1) * block)
            mixed = jnp.dot(masked, normed[at], preferred_element_type=F32) + offset
            done = (gated_ref[at] * mixed).astype(BF16)
            for k in range(copies):
                out_ref[k, at] = done

    return pl.pallas_call(
        body,
        out_shape=pltpu.VMEM((copies, rows, channels), BF16),
        in_specs=[whole_vmem()] * 6,
        out_specs=whole_vmem(),
        compiler_params=pltpu.CompilerParams(vmem_limit_bytes=12 << 20),
        cost_estimate=pl.CostEstimate(flops=2 * rows * block * channels, bytes_accessed=2 << 20, transcendentals=rows),
        name="gated_copies",
    )(in_vmem(known), in_vmem(gated), in_vmem(valued), gain.reshape(1, channels), weight, bias)


def projected(place, gated, pieces):
    chips, rows, channels = gated.shape
    peers = len(pieces)
    depth = 32
    zs = pieces[0].shape[0] // chips // depth
    width = zs * peers * depth
    steps = 8
    deep = zs // steps
    span = width // steps
    ahead = 3

    def body(place_ref, gated_ref, *rest):
        pieces = rest[:peers]
        out_ref, weights, left, sems = rest[peers:]
        y = place_ref[2]
        copies = []
        for j in range(steps):
            at_z = pl.ds(j * deep, deep)
            some = []
            for n in range(peers):
                at_y = lax.rem(y + peers - n, peers)
                some.append(pltpu.make_async_copy(pieces[n].at[:, at_z], weights.at[:, at_z, at_y], sems.at[j, n]))
            copies.append(some)
        for some in copies[:ahead]:
            for c in some:
                c.start()
        for k in range(chips):
            left[:, k * channels : (k + 1) * channels] = gated_ref[k]
        for j in range(steps):
            for c in copies[j]:
                c.wait()
            if j + ahead < steps:
                for c in copies[j + ahead]:
                    c.start()
            right = [weights[k, j * deep : (j + 1) * deep].reshape(span, channels) for k in range(chips)]
            right = jnp.concatenate(right, axis=1)
            part = lax.dot_general(left[...], right, ACROSS, preferred_element_type=F32)
            out_ref[:, j * span : (j + 1) * span] = part.astype(BF16)

    given = [p.reshape(chips, zs, depth, channels) for p in pieces]
    anywhere = pl.BlockSpec(memory_space=pl.ANY)
    return pl.pallas_call(
        body,
        out_shape=jax.ShapeDtypeStruct((rows, width), BF16),
        in_specs=[pl.BlockSpec(memory_space=pltpu.SMEM), whole_vmem()] + [anywhere] * peers,
        out_specs=whole_vmem(),
        scratch_shapes=[
            pltpu.VMEM((chips, zs, peers, depth, channels), BF16),
            pltpu.VMEM((rows, chips * channels), BF16),
            pltpu.SemaphoreType.DMA((steps, peers)),
        ],
        cost_estimate=pl.CostEstimate(flops=2 * rows * width * chips * channels, bytes_accessed=6 << 20, transcendentals=0),
        name="projected",
    )(in_hbm(place), in_vmem(gated), *given)


def mixer(place, own, other, blocks, gain, ffw, ff):
    rows, width = own.shape
    parts, _, feats = blocks.shape
    chips = parts // 2
    half = rows // 2
    few = rows // parts
    edges = [0, 384, 768, 1152, 2 * ff, 3 * ff]
    spans = [e - b for b, e in zip(edges, edges[1:])]
    chunks = len(spans)
    ahead = 3
    step = 256
    lanes = 128

    def body(place_ref, own_ref, other_ref, blocks_ref, gain_ref, ffw_ref, mine_ref, hidden_ref, give_ref, *rest):
        weights = rest[:chunks]
        base, low, vals, left, acc, in_sems, sems = rest[chunks:]
        core = place_ref[0]
        me = place_ref[1]
        inputs = []
        for j in range(parts):
            at = pl.ds(j * feats, feats)
            inputs.append(
                [
                    pltpu.make_async_copy(own_ref.at[:, at], low.at[j], in_sems.at[j, 0]),
                    pltpu.make_async_copy(blocks_ref.at[j], base.at[j], in_sems.at[j, 1]),
                ]
            )
            for c in inputs[j]:
                c.start()
        copies = []
        for n in range(chunks):
            at = pl.ds(edges[n], spans[n])
            copies.append(pltpu.make_async_copy(ffw_ref.at[:, at], weights[n], sems.at[n]))
        for c in copies[:ahead]:
            c.start()
        total = jnp.zeros((rows, lanes), F32)
        squares = jnp.zeros((rows, lanes), F32)
        for j in range(parts):
            for c in inputs[j]:
                c.wait()
            for b in range(0, feats, lanes):
                high = other_ref[:, j * feats + b : j * feats + b + lanes]
                mix = (low[j, :, b : b + lanes].astype(F32) + high.astype(F32)).astype(BF16)
                these = ALPHA * base[j, :, b : b + lanes].astype(F32) + mix.astype(F32)
                vals[j, :, b : b + lanes] = these
                total += these
                squares += these * these
        mean = jnp.sum(total, axis=1, keepdims=True) / width
        scale = lax.rsqrt(jnp.sum(squares, axis=1, keepdims=True) / width - mean * mean + EPS)
        for j in range(parts):
            at = slice(j * feats, (j + 1) * feats)
            left[:, at] = ((vals[j] - mean) * scale * gain_ref[:, at]).astype(BF16)
        mine_ref[...] = left[pl.ds(pl.multiple_of(me * few, few), few), :]
        for n in range(chunks - 1):
            copies[n].wait()
            if n + ahead < chunks:
                copies[n + ahead].start()
            acc[:, edges[n] : edges[n + 1]] = jnp.dot(left[...], weights[n][...], preferred_element_type=F32)
        gate = acc[:, :ff]
        hidden = (gate * lax.logistic(gate) * acc[:, ff:]).astype(BF16)
        copies[-1].wait()

        def rows_of(which):
            return jnp.concatenate([hidden[(2 * x + which) * few : (2 * x + which + 1) * few] for x in range(chips)], axis=0)

        def out(keep_core):
            hidden_ref[...] = rows_of(keep_core)
            given = rows_of(1 - keep_core)
            for b in range(0, width, step):
                done = lax.dot_general(given, weights[-1][b : b + step], ACROSS, preferred_element_type=F32)
                give_ref[:, b : b + step] = done.astype(BF16)

        @pl.when(core == 0)
        def _():
            out(0)

        @pl.when(core == 1)
        def _():
            out(1)

    anywhere = pl.BlockSpec(memory_space=pltpu.HBM)
    return pl.pallas_call(
        body,
        out_shape=(
            pltpu.VMEM((few, width), BF16),
            pltpu.VMEM((half, ff), BF16),
            pltpu.VMEM((half, width), BF16),
        ),
        in_specs=[pl.BlockSpec(memory_space=pltpu.SMEM), anywhere, whole_vmem(), anywhere, whole_vmem(), anywhere],
        out_specs=(whole_vmem(),) * 3,
        scratch_shapes=[
            *(pltpu.VMEM((width, n), BF16) for n in spans),
            pltpu.VMEM((parts, rows, feats), BF16),
            pltpu.VMEM((parts, rows, feats), BF16),
            pltpu.VMEM((parts, rows, feats), F32),
            pltpu.VMEM((rows, width), BF16),
            pltpu.VMEM((rows, 2 * ff), F32),
            pltpu.SemaphoreType.DMA((parts, 2)),
            pltpu.SemaphoreType.DMA((chunks,)),
        ],
        cost_estimate=pl.CostEstimate(flops=6 * rows * width * ff, bytes_accessed=18 << 20, transcendentals=rows * ff),
        name="mixer",
        compiler_params=pltpu.CompilerParams(vmem_limit_bytes=40 << 20),
    )(in_hbm(place), in_hbm(own), in_vmem(other), in_hbm(blocks), gain.reshape(1, width), in_hbm(ffw))


def kept(hidden, ffw):
    half, ff = hidden.shape
    width = ffw.shape[0]
    steps = 4
    span = width // steps

    def body(hidden_ref, ffw_ref, out_ref, weights, sems):
        copies = []
        for n in range(steps):
            at = pl.ds(n * span, span)
            copies.append(pltpu.make_async_copy(ffw_ref.at[at, pl.ds(2 * ff, ff)], weights.at[at], sems.at[n]))
            copies[n].start()
        for n in range(steps):
            copies[n].wait()
            at = slice(n * span, (n + 1) * span)
            done = lax.dot_general(hidden_ref[...], weights[at], ACROSS, preferred_element_type=F32)
            out_ref[:, at] = done.astype(BF16)

    return pl.pallas_call(
        body,
        out_shape=pltpu.VMEM((half, width), BF16),
        in_specs=[whole_vmem(), pl.BlockSpec(memory_space=pltpu.HBM)],
        out_specs=whole_vmem(),
        scratch_shapes=[pltpu.VMEM((width, ff), BF16), pltpu.SemaphoreType.DMA((steps,))],
        compiler_params=pltpu.CompilerParams(vmem_limit_bytes=12 << 20),
        cost_estimate=pl.CostEstimate(flops=2 * half * width * ff, bytes_accessed=4 << 20, transcendentals=0),
        name="kept",
    )(in_vmem(hidden), in_hbm(ffw))


def from_each(value, axis):
    size = lax.axis_size(axis)
    return [value] + [lax.ppermute(value, axis, [(i, (i + k) % size) for i in range(size)]) for k in range(1, size)]


def on_device(
    tokens,
    u_weight,
    v_weight,
    sg_gain,
    spatial_weight,
    spatial_bias,
    out_weight,
    gain_one,
    gate_weight,
    up_weight,
    down_weight,
    gain_two,
):
    core = lax.axis_index("c")
    chips = lax.axis_size("x")
    parts = chips * lax.axis_size("c")
    rows, feats = tokens.shape
    width = feats * parts
    sg = u_weight.shape[1]
    own_rows = rows // parts

    blocks = sent_to_all(tokens, TP)

    ffw = sent_to_all(jnp.concatenate([gate_weight, up_weight, down_weight.T], axis=1), "y")
    ffw = ffw.reshape(-1, ffw.shape[2])
    ffw = lax.all_gather(ffw, "z", axis=0, tiled=True)

    small = jnp.concatenate([u_weight, v_weight, out_weight.T], axis=1)
    small = lax.all_gather(small, "z", axis=0, tiled=True)
    gates = sent_to_all(small[:, : 2 * sg], "y")
    out_x = lax.all_gather(small[:, 2 * sg :], "x", axis=0, tiled=True)
    out_rows = from_each(out_x, "y")

    gains = jnp.concatenate([gain_one, gain_two]).reshape(1, rows)
    gated, valued, sums = branches(blocks, gates, gains)
    known = lax.all_to_all(sums, TP, 0, 0, tiled=True)
    gains = known[:, 2].reshape(parts, 2, feats)
    gain_1 = gains[:, 0].reshape(width)
    gain_2 = gains[:, 1].reshape(width)
    copies = gated_copies(known, gated, valued, sg_gain, spatial_weight, spatial_bias, chips)
    together = lax.all_to_all(copies, "x", 0, 0, tiled=True)
    place = jnp.stack([core, lax.axis_index(TP), lax.axis_index("y")]).astype(jnp.int32)
    own = projected(place, together, out_rows)
    mine, hidden, give = mixer(place, own, to_partner(own), blocks, gain_1, ffw, gate_weight.shape[1])
    keep = kept(hidden, ffw)
    pair = (keep.astype(F32) + to_partner(give).astype(F32)).astype(BF16)
    pieces = lax.all_to_all(pair.reshape(chips, own_rows, width), "x", 0, 0, tiled=True)
    last = last_norm(pieces, mine, gain_2, parts)
    return lax.all_to_all(last, TP, 0, 0, tiled=True).reshape(rows, feats)


def solution(mesh):
    tp = mesh.shape["tp"]
    finer = Mesh(mesh.devices.reshape(16, 4, tp // 2, 2), ("z", "y", "x", "c"))
    return jax.shard_map(
        on_device,
        mesh=finer,
        in_specs=(
            P(FS, TP),
            P(FS, TP),
            P(FS, TP),
            P(TP),
            P(TP, None, None),
            P(TP, None),
            P(TP, FS),
            P(TP),
            P(FS, TP),
            P(FS, TP),
            P(TP, FS),
            P(TP),
        ),
        out_specs=P(FS, TP),
        check_vma=False,
    )
```

```python
import jax
import jax.numpy as jnp
from jax import lax
from jax.experimental import pallas as pl
from jax.experimental.pallas import tpu as pltpu
from jax.sharding import Mesh
from jax.sharding import PartitionSpec as P

FS = ("z", "y")
TP = ("x", "c")

EPS = 1e-05
ALPHA = 2.0**0.25
BF16 = jnp.bfloat16
F32 = jnp.float32
ACROSS = (((1,), (1,)), ((), ()))


def sent_to_all(value, axis):
    copies = jnp.broadcast_to(value, (lax.axis_size(axis), *value.shape))
    return lax.all_to_all(copies, axis, split_axis=0, concat_axis=0, tiled=True)


def to_partner(value):
    return lax.ppermute(value, "c", [(0, 1), (1, 0)])


def row_norm(vals, gain):
    count = vals.shape[1]
    mean = jnp.sum(vals, axis=1, keepdims=True) / count
    square = jnp.sum(vals * vals, axis=1, keepdims=True) / count
    return (vals - mean) * lax.rsqrt(square - mean * mean + EPS) * gain


def in_vmem(value):
    return pltpu.with_memory_space_constraint(value, pltpu.VMEM)


def in_hbm(value):
    return pltpu.with_memory_space_constraint(value, pltpu.HBM)


def whole_vmem():
    return pl.BlockSpec(memory_space=pltpu.VMEM)


def last_norm(pieces, base, gain, parts):
    peers, rows, width = pieces.shape

    def body(pieces_ref, base_ref, gain_ref, out_ref):
        added = pieces_ref[0].astype(F32)
        for k in range(1, peers):
            added = added + pieces_ref[k].astype(F32)
        vals = ALPHA * base_ref[...].astype(F32) + added.astype(BF16).astype(F32)
        done = row_norm(vals, gain_ref[...]).astype(BF16)
        for k in range(parts):
            out_ref[k] = done[:, k * (width // parts) : (k + 1) * (width // parts)]

    return pl.pallas_call(
        body,
        out_shape=pltpu.VMEM((parts, rows, width // parts), BF16),
        in_specs=[whole_vmem()] * 3,
        out_specs=whole_vmem(),
        name="last_norm",
    )(in_vmem(pieces), in_vmem(base), gain.reshape(1, width))


def branches(blocks, gates, gains):
    parts, rows, feats = blocks.shape
    ys, deep, columns = gates.shape
    width = parts * feats
    half = columns // 2
    depth = 32

    def body(blocks_ref, gates_ref, gains_ref, gated_ref, valued_ref, sums_ref, left, right, sems):
        copies = []
        for k in range(parts):
            copies.append(pltpu.make_async_copy(blocks_ref.at[k], left.at[:, pl.ds(k * feats, feats)], sems.at[k]))
            copies[k].start()
        for z in range(deep // depth):
            for y in range(ys):
                at = (z * ys + y) * depth
                right[at : at + depth] = gates_ref[y, z * depth : (z + 1) * depth]
        for c in copies:
            c.wait()
        both = jnp.dot(left[...], right[...], preferred_element_type=F32)
        gated_ref[...] = jax.nn.gelu(both[:, :half])
        valued = jax.nn.gelu(both[:, half:])
        valued_ref[...] = valued
        turned = valued.T
        total = jnp.sum(turned, axis=0, keepdims=True)
        squares = jnp.sum(turned * turned, axis=0, keepdims=True)
        for k in range(parts):
            sums_ref[k, 0:1] = total
            sums_ref[k, 1:2] = squares
            sums_ref[k, 2:3] = gains_ref[...]
            sums_ref[k, 3:4] = gains_ref[...]

    return pl.pallas_call(
        body,
        out_shape=(
            pltpu.VMEM((rows, half), F32),
            pltpu.VMEM((rows, half), F32),
            pltpu.VMEM((parts, 4, rows), F32),
        ),
        in_specs=[pl.BlockSpec(memory_space=pltpu.HBM), whole_vmem(), whole_vmem()],
        out_specs=(whole_vmem(),) * 3,
        scratch_shapes=[
            pltpu.VMEM((rows, width), BF16),
            pltpu.VMEM((width, columns), BF16),
            pltpu.SemaphoreType.DMA((parts,)),
        ],
        compiler_params=pltpu.CompilerParams(vmem_limit_bytes=24 << 20),
        cost_estimate=pl.CostEstimate(flops=2 * rows * width * columns, bytes_accessed=4 << 20, transcendentals=2 * rows * columns),
        name="branches",
    )(in_hbm(blocks), in_vmem(gates), gains)


def gated_copies(known, gated, valued, gain, weight, bias, copies):
    parts, _, rows = known.shape
    channels = gated.shape[1]
    block = weight.shape[1]
    count = parts * channels

    def body(known_ref, gated_ref, valued_ref, gain_ref, weight_ref, bias_ref, out_ref):
        sums = known_ref[0]
        for k in range(1, parts):
            sums = sums + known_ref[k]
        mean = sums[0:1] / count
        square = sums[1:2] / count
        scale = lax.rsqrt(square - mean * mean + EPS)
        mean = jnp.broadcast_to(mean, (channels, rows)).T
        scale = jnp.broadcast_to(scale, (channels, rows)).T
        normed = ((valued_ref[...] - mean) * scale * gain_ref[...]).astype(BF16)
        row = lax.broadcasted_iota(jnp.int32, (block, block), 0)
        column = lax.broadcasted_iota(jnp.int32, (block, block), 1)
        masked = jnp.where(row >= column, weight_ref[0].astype(F32), 0.0).astype(BF16)
        offset = jnp.broadcast_to(bias_ref[...], (channels, block)).T
        for n in range(rows // block):
            at = slice(n * block, (n + 1) * block)
            mixed = jnp.dot(masked, normed[at], preferred_element_type=F32) + offset
            done = (gated_ref[at] * mixed).astype(BF16)
            for k in range(copies):
                out_ref[k, at] = done

    return pl.pallas_call(
        body,
        out_shape=pltpu.VMEM((copies, rows, channels), BF16),
        in_specs=[whole_vmem()] * 6,
        out_specs=whole_vmem(),
        compiler_params=pltpu.CompilerParams(vmem_limit_bytes=12 << 20),
        cost_estimate=pl.CostEstimate(flops=2 * rows * block * channels, bytes_accessed=2 << 20, transcendentals=rows),
        name="gated_copies",
    )(in_vmem(known), in_vmem(gated), in_vmem(valued), gain.reshape(1, channels), weight, bias)


def projected(place, gated, pieces):
    chips, rows, channels = gated.shape
    peers = len(pieces)
    depth = 32
    zs = pieces[0].shape[0] // chips // depth
    width = zs * peers * depth
    steps = 8
    deep = zs // steps
    span = width // steps
    ahead = 3

    def body(place_ref, gated_ref, *rest):
        pieces = rest[:peers]
        out_ref, weights, left, sems = rest[peers:]
        y = place_ref[2]
        copies = []
        for j in range(steps):
            at_z = pl.ds(j * deep, deep)
            some = []
            for n in range(peers):
                at_y = lax.rem(y + peers - n, peers)
                some.append(pltpu.make_async_copy(pieces[n].at[:, at_z], weights.at[:, at_z, at_y], sems.at[j, n]))
            copies.append(some)
        for some in copies[:ahead]:
            for c in some:
                c.start()
        for k in range(chips):
            left[:, k * channels : (k + 1) * channels] = gated_ref[k]
        for j in range(steps):
            for c in copies[j]:
                c.wait()
            if j + ahead < steps:
                for c in copies[j + ahead]:
                    c.start()
            right = [weights[k, j * deep : (j + 1) * deep].reshape(span, channels) for k in range(chips)]
            right = jnp.concatenate(right, axis=1)
            part = lax.dot_general(left[...], right, ACROSS, preferred_element_type=F32)
            out_ref[:, j * span : (j + 1) * span] = part.astype(BF16)

    given = [p.reshape(chips, zs, depth, channels) for p in pieces]
    anywhere = pl.BlockSpec(memory_space=pl.ANY)
    return pl.pallas_call(
        body,
        out_shape=jax.ShapeDtypeStruct((rows, width), BF16),
        in_specs=[pl.BlockSpec(memory_space=pltpu.SMEM), whole_vmem()] + [anywhere] * peers,
        out_specs=whole_vmem(),
        scratch_shapes=[
            pltpu.VMEM((chips, zs, peers, depth, channels), BF16),
            pltpu.VMEM((rows, chips * channels), BF16),
            pltpu.SemaphoreType.DMA((steps, peers)),
        ],
        cost_estimate=pl.CostEstimate(flops=2 * rows * width * chips * channels, bytes_accessed=6 << 20, transcendentals=0),
        name="projected",
    )(in_hbm(place), in_vmem(gated), *given)


def mixer(place, own, other, blocks, gain, ffw, ff):
    rows, width = own.shape
    parts, _, feats = blocks.shape
    chips = parts // 2
    half = rows // 2
    few = rows // parts
    edges = [0, 384, 768, 1152, 2 * ff, 3 * ff]
    spans = [e - b for b, e in zip(edges, edges[1:])]
    chunks = len(spans)
    ahead = 3
    step = 256
    lanes = 128

    def body(place_ref, own_ref, other_ref, blocks_ref, gain_ref, ffw_ref, mine_ref, hidden_ref, give_ref, *rest):
        weights = rest[:chunks]
        base, low, vals, left, acc, in_sems, sems = rest[chunks:]
        core = place_ref[0]
        me = place_ref[1]
        inputs = []
        for j in range(parts):
            at = pl.ds(j * feats, feats)
            inputs.append(
                [
                    pltpu.make_async_copy(own_ref.at[:, at], low.at[j], in_sems.at[j, 0]),
                    pltpu.make_async_copy(blocks_ref.at[j], base.at[j], in_sems.at[j, 1]),
                ]
            )
            for c in inputs[j]:
                c.start()
        copies = []
        for n in range(chunks):
            at = pl.ds(edges[n], spans[n])
            copies.append(pltpu.make_async_copy(ffw_ref.at[:, at], weights[n], sems.at[n]))
        for c in copies[:ahead]:
            c.start()
        total = jnp.zeros((rows, lanes), F32)
        squares = jnp.zeros((rows, lanes), F32)
        for j in range(parts):
            for c in inputs[j]:
                c.wait()
            for b in range(0, feats, lanes):
                high = other_ref[:, j * feats + b : j * feats + b + lanes]
                mix = (low[j, :, b : b + lanes].astype(F32) + high.astype(F32)).astype(BF16)
                these = ALPHA * base[j, :, b : b + lanes].astype(F32) + mix.astype(F32)
                vals[j, :, b : b + lanes] = these
                total += these
                squares += these * these
        mean = jnp.sum(total, axis=1, keepdims=True) / width
        scale = lax.rsqrt(jnp.sum(squares, axis=1, keepdims=True) / width - mean * mean + EPS)
        for j in range(parts):
            at = slice(j * feats, (j + 1) * feats)
            left[:, at] = ((vals[j] - mean) * scale * gain_ref[:, at]).astype(BF16)
        mine_ref[...] = left[pl.ds(pl.multiple_of(me * few, few), few), :]
        for n in range(chunks - 1):
            copies[n].wait()
            if n + ahead < chunks:
                copies[n + ahead].start()
            acc[:, edges[n] : edges[n + 1]] = jnp.dot(left[...], weights[n][...], preferred_element_type=F32)
        gate = acc[:, :ff]
        hidden = (gate * lax.logistic(gate) * acc[:, ff:]).astype(BF16)
        copies[-1].wait()

        def rows_of(which):
            return jnp.concatenate([hidden[(2 * x + which) * few : (2 * x + which + 1) * few] for x in range(chips)], axis=0)

        def out(keep_core):
            hidden_ref[...] = rows_of(keep_core)
            given = rows_of(1 - keep_core)
            for b in range(0, width, step):
                done = lax.dot_general(given, weights[-1][b : b + step], ACROSS, preferred_element_type=F32)
                give_ref[:, b : b + step] = done.astype(BF16)

        @pl.when(core == 0)
        def _():
            out(0)

        @pl.when(core == 1)
        def _():
            out(1)

    anywhere = pl.BlockSpec(memory_space=pltpu.HBM)
    return pl.pallas_call(
        body,
        out_shape=(
            pltpu.VMEM((few, width), BF16),
            pltpu.VMEM((half, ff), BF16),
            pltpu.VMEM((half, width), BF16),
        ),
        in_specs=[pl.BlockSpec(memory_space=pltpu.SMEM), anywhere, whole_vmem(), anywhere, whole_vmem(), anywhere],
        out_specs=(whole_vmem(),) * 3,
        scratch_shapes=[
            *(pltpu.VMEM((width, n), BF16) for n in spans),
            pltpu.VMEM((parts, rows, feats), BF16),
            pltpu.VMEM((parts, rows, feats), BF16),
            pltpu.VMEM((parts, rows, feats), F32),
            pltpu.VMEM((rows, width), BF16),
            pltpu.VMEM((rows, 2 * ff), F32),
            pltpu.SemaphoreType.DMA((parts, 2)),
            pltpu.SemaphoreType.DMA((chunks,)),
        ],
        cost_estimate=pl.CostEstimate(flops=6 * rows * width * ff, bytes_accessed=18 << 20, transcendentals=rows * ff),
        name="mixer",
        compiler_params=pltpu.CompilerParams(vmem_limit_bytes=40 << 20),
    )(in_hbm(place), in_hbm(own), in_vmem(other), in_hbm(blocks), gain.reshape(1, width), in_hbm(ffw))


def kept(hidden, ffw):
    half, ff = hidden.shape
    width = ffw.shape[0]
    steps = 4
    span = width // steps

    def body(hidden_ref, ffw_ref, out_ref, weights, sems):
        copies = []
        for n in range(steps):
            at = pl.ds(n * span, span)
            copies.append(pltpu.make_async_copy(ffw_ref.at[at, pl.ds(2 * ff, ff)], weights.at[at], sems.at[n]))
            copies[n].start()
        for n in range(steps):
            copies[n].wait()
            at = slice(n * span, (n + 1) * span)
            done = lax.dot_general(hidden_ref[...], weights[at], ACROSS, preferred_element_type=F32)
            out_ref[:, at] = done.astype(BF16)

    return pl.pallas_call(
        body,
        out_shape=pltpu.VMEM((half, width), BF16),
        in_specs=[whole_vmem(), pl.BlockSpec(memory_space=pltpu.HBM)],
        out_specs=whole_vmem(),
        scratch_shapes=[pltpu.VMEM((width, ff), BF16), pltpu.SemaphoreType.DMA((steps,))],
        compiler_params=pltpu.CompilerParams(vmem_limit_bytes=12 << 20),
        cost_estimate=pl.CostEstimate(flops=2 * half * width * ff, bytes_accessed=4 << 20, transcendentals=0),
        name="kept",
    )(in_vmem(hidden), in_hbm(ffw))


def sent_on(value, axis, steps):
    size = lax.axis_size(axis)
    return lax.ppermute(value, axis, [(i, (i + steps) % size) for i in range(size)])


def on_device(
    tokens,
    u_weight,
    v_weight,
    sg_gain,
    spatial_weight,
    spatial_bias,
    out_weight,
    gain_one,
    gate_weight,
    up_weight,
    down_weight,
    gain_two,
):
    core = lax.axis_index("c")
    chips = lax.axis_size("x")
    parts = chips * lax.axis_size("c")
    rows, feats = tokens.shape
    width = feats * parts
    sg = u_weight.shape[1]
    own_rows = rows // parts

    blocks = sent_to_all(tokens, TP)

    ffw = sent_to_all(jnp.concatenate([gate_weight, up_weight, down_weight.T], axis=1), "y")
    ffw = ffw.reshape(-1, ffw.shape[2])
    ffw = lax.all_gather(ffw, "z", axis=0, tiled=True)

    small = jnp.concatenate([u_weight, v_weight, out_weight.T], axis=1)
    small = lax.all_gather(small, "z", axis=0, tiled=True)
    gates = sent_to_all(small[:, : 2 * sg], "y")
    out_x = lax.all_gather(small[:, 2 * sg :], "x", axis=0, tiled=True)
    near = [sent_on(out_x, "y", k) for k in (1, 3)]
    far = sent_on(out_x, "y", 2)
    out_rows = [out_x, near[0], far, near[1]]

    gains = jnp.concatenate([gain_one, gain_two]).reshape(1, rows)
    gated, valued, sums = branches(blocks, gates, gains)
    known = lax.all_to_all(sums, TP, 0, 0, tiled=True)
    gains = known[:, 2].reshape(parts, 2, feats)
    gain_1 = gains[:, 0].reshape(width)
    gain_2 = gains[:, 1].reshape(width)
    copies = gated_copies(known, gated, valued, sg_gain, spatial_weight, spatial_bias, chips)
    together = lax.all_to_all(copies, "x", 0, 0, tiled=True)
    place = jnp.stack([core, lax.axis_index(TP), lax.axis_index("y")]).astype(jnp.int32)
    own = projected(place, together, out_rows)
    mine, hidden, give = mixer(place, own, to_partner(own), blocks, gain_1, ffw, gate_weight.shape[1])
    keep = kept(hidden, ffw)
    pair = (keep.astype(F32) + to_partner(give).astype(F32)).astype(BF16)
    pieces = lax.all_to_all(pair.reshape(chips, own_rows, width), "x", 0, 0, tiled=True)
    last = last_norm(pieces, mine, gain_2, parts)
    return lax.all_to_all(last, TP, 0, 0, tiled=True).reshape(rows, feats)


def solution(mesh):
    tp = mesh.shape["tp"]
    finer = Mesh(mesh.devices.reshape(16, 4, tp // 2, 2), ("z", "y", "x", "c"))
    return jax.shard_map(
        on_device,
        mesh=finer,
        in_specs=(
            P(FS, TP),
            P(FS, TP),
            P(FS, TP),
            P(TP),
            P(TP, None, None),
            P(TP, None),
            P(TP, FS),
            P(TP),
            P(FS, TP),
            P(FS, TP),
            P(TP, FS),
            P(TP),
        ),
        out_specs=P(FS, TP),
        check_vma=False,
    )
```
